128 devices in a mesh: ep: 128 (over z, y, x, core).
Axes of the slice: x: 4, y: 4, z: 4, core: 2. Of those that a mesh axis runs over, the one named last changes fastest.
Arguments:
- tokens: bfloat16 [1024, 2048], P('ep'), may hold values from -6 to 6
- premix_gain: float32 [2048], replicated, may hold values from 0.1 to 1.9
- postmix_gain: float32 [2048], replicated, may hold values from 0.1 to 1.9
- prefeed_gain: float32 [2048], replicated, may hold values from 0.1 to 1.9
- postfeed_gain: float32 [2048], replicated, may hold values from 0.1 to 1.9
- query_weight: bfloat16 [2048, 1024], P('ep'), may hold values from -0.125 to 0.125
- key_weight: bfloat16 [2048, 1024], P('ep'), may hold values from -0.125 to 0.125
- value_weight: bfloat16 [2048, 1024], P('ep'), may hold values from -0.125 to 0.125
- outgate_weight: bfloat16 [2048, 1024], P('ep'), may hold values from -0.125 to 0.125
- ingate_weight: bfloat16 [2048, 8], replicated, may hold values from -0.125 to 0.125
- forget_weight: bfloat16 [2048, 8], replicated, may hold values from -0.125 to 0.125
- ingate_bias: float32 [8], replicated, may hold values from -1 to 1
- forget_bias: float32 [8], replicated, may hold values from -1 to 5
- memory_state: float32 [1024, 8, 128, 128], P('ep'), may hold values from -1.25 to 1.25
- normalizer: float32 [1024, 8, 128], P('ep'), may hold values from -1.75 to 1.75
- stabilizer: float32 [1024, 8], P('ep'), may hold values from -2 to 2
- output_weight: bfloat16 [1024, 2048], P(None, 'ep'), may hold values from -0.1875 to 0.1875
- expert_ids: int32 [1024, 6], P('ep'), may hold values from 0 to 127, all different within a row; in each aligned block of 8 rows (0 to 7, 8 to 15, ...) at most 2 rows name the same one
- route_weights: float32 [1024, 6], P('ep'), may hold values from 0.2 to 0.8
- expert_gate: bfloat16 [128, 2048, 512], P('ep'), may hold values from -0.125 to 0.125
- expert_up: bfloat16 [128, 2048, 512], P('ep'), may hold values from -0.125 to 0.125
- expert_down: bfloat16 [128, 512, 2048], P('ep'), may hold values from -0.25 to 0.25
- shared_gate: bfloat16 [2048, 512], replicated, may hold values from -0.125 to 0.125
- shared_up: bfloat16 [2048, 512], replicated, may hold values from -0.125 to 0.125
- shared_down: bfloat16 [512, 2048], replicated, may hold values from -0.25 to 0.25
Outputs:
- next_tokens: bfloat16 [1024, 2048], P('ep')
- next_memory: float32 [1024, 8, 128, 128], P('ep')
- next_normalizer: float32 [1024, 8, 128], P('ep')
- next_stabilizer: float32 [1024, 8], P('ep')
The draws below stay inside these ranges and needn't reach their ends.
Inputs may be any that keep to these rules, and one draw needn't show every extreme that they name: `expert_ids`: each row names 6 different experts. Among the rows of one device no expert is named more than 2 times, and in every draw some expert is named exactly 2 times by the rows of some device.
All inputs are finite; a program needn't handle non-finite values.
Results may differ from the reference program's by a relative error of at most 0.0097.
Values may be sent and summed in bfloat16 or wider, within the bound.
A program may use at most 128 MiB of HBM per device.

```python
import math
import jax
import jax.numpy as jnp
import numpy as np
from jax import lax

D = 2048
HEADS = 8
HEAD_DIM = 128
D_MEM = 1024
FF = 512
TOP_K = 6
EXPERTS = 128
SEQ_DEV = 8
SEQS = 1024
CAP = 2
N_EP = 128


def block_scale(stream_key, extent, split, smallest, top_value):
    factor_of, own = 1.0, jax.random.fold_in(stream_key, 6)
    for axis_at, shards_of in split:
        heights = jnp.exp(jax.random.uniform(jax.random.fold_in(own, axis_at), (shards_of,), jnp.float32, smallest / len(split), top_value / len(split)))
        factor_of = factor_of * jnp.repeat(heights, extent[axis_at] // shards_of).reshape([-1 if axis == axis_at else 1 for axis in range(len(extent))])
    return factor_of


def deal_out(rng, own, number, rows, number_of, top, limit, slope):
    sequence = jax.random.permutation(rng, number_of)
    crowded, usual = portions_of(number_of, rows * top, limit, slope, True), portions_of(number_of, rows * top, limit, slope, False)
    places = jnp.arange(number_of)

    def named(lengths, rotation):
        used = int((lengths > 0).sum())
        fixed = max(1, used // 4)
        shifted = fixed + (places - fixed + rotation * (used - fixed)) % max(1, number_of - fixed)
        return jnp.zeros((number_of,), jnp.int32).at[sequence[jnp.where(places < fixed, places, shifted)]].set(jnp.asarray(lengths, jnp.int32))

    lengths = jnp.where(number % 4 == 0, named(crowded, number // 4), named(usual, number - number // 4 - 1))
    mixed = jax.random.permutation(jax.random.fold_in(own, 3), number_of)
    donor, taker = mixed[0:number_of // 2 * 2:2], mixed[1:number_of // 2 * 2:2]
    margin = jnp.minimum(lengths[donor] - 1, limit - lengths[taker]) // 2
    margin = jnp.where((donor == sequence[0]) | (taker == sequence[0]) | (lengths[taker] == 0), 0, jnp.maximum(margin, 0))
    shifted = jax.random.randint(jax.random.fold_in(own, 4), (number_of // 2,), 0, 1 << 20) % (margin + 1)
    lengths = lengths.at[donor].add(-shifted).at[taker].add(shifted)
    labels = jnp.searchsorted(jnp.cumsum(lengths), jnp.arange(rows * top), side="right").astype(jnp.int32)
    listing = labels.reshape(top, rows).T
    listing = listing[jax.random.permutation(jax.random.fold_in(own, 1), rows)]
    rotation = jax.random.randint(jax.random.fold_in(own, 2), (rows, 1), 0, top)
    return jnp.take_along_axis(listing, (jnp.arange(top)[None, :] + rotation) % top, axis=1)


def portions_of(number_of, total, limit, skew, full):
    weights = [(1 << 20) // math.isqrt(rank ** skew) + 1 for rank in range(1, number_of + 1)]
    largest = limit if full else min(limit, max(-(-total // number_of), total * weights[0] // sum(weights)))
    least = 1 if total - largest >= number_of - 1 else 0
    given, rest = [largest] + [least] * (number_of - 1), total - largest - least * (number_of - 1)
    while rest > 0:
        free = [i for i in range(1, number_of) if given[i] < largest] or [i for i in range(1, number_of) if given[i] < limit]
        pool, left = sum([weights[i] for i in free]), rest
        for i in free:
            addition = min(limit - given[i], max(1, left * weights[i] // pool), rest)
            given[i] = given[i] + addition
            rest = rest - addition
    return np.array(given)


def noise(own_key, extent, scale, bound, shards=(), kind=jnp.bfloat16):
    result = scale * jax.random.normal(own_key, extent, jnp.float32)
    if shards:
        result = result * block_scale(own_key, extent, shards, -0.22, 0.18)
    return jnp.clip(result, -bound, bound).astype(kind)


def setup_inputs(seed: int = 0) -> dict:
    streams_of = jax.random.split(jax.random.key(seed), 26)
    tokens = noise(streams_of[0], (SEQS, D), 1.0, 6.0, ((0, 128),))
    premix_gain = jnp.clip(1.0 + 0.18 * jax.random.normal(streams_of[1], (D,), jnp.float32), 0.1, 1.9)
    postmix_gain = jnp.clip(1.0 + 0.18 * jax.random.normal(streams_of[2], (D,), jnp.float32), 0.1, 1.9)
    prefeed_gain = jnp.clip(1.0 + 0.18 * jax.random.normal(streams_of[3], (D,), jnp.float32), 0.1, 1.9)
    postfeed_gain = jnp.clip(1.0 + 0.18 * jax.random.normal(streams_of[4], (D,), jnp.float32), 0.1, 1.9)
    query_weight = noise(streams_of[5], (D, D_MEM), D ** -0.5, 0.125, ((0, 128),))
    key_weight = noise(streams_of[6], (D, D_MEM), D ** -0.5, 0.125, ((0, 128),))
    value_weight = noise(streams_of[7], (D, D_MEM), D ** -0.5, 0.125, ((0, 128),))
    outgate_weight = noise(streams_of[8], (D, D_MEM), D ** -0.5, 0.125, ((0, 128),))
    ingate_weight = noise(streams_of[9], (D, HEADS), D ** -0.5, 0.125)
    forget_weight = noise(streams_of[10], (D, HEADS), D ** -0.5, 0.125)
    ingate_bias = jnp.clip(jax.random.uniform(streams_of[11], (HEADS,), jnp.float32, -1.0, 1.0), -1.0, 1.0)
    forget_bias = jnp.clip(jax.random.uniform(streams_of[12], (HEADS,), jnp.float32, -1.0, 5.0), -1.0, 5.0)
    memory_state = noise(streams_of[13], (SEQS, HEADS, HEAD_DIM, HEAD_DIM), 0.2, 1.25, ((0, 128),), jnp.float32)
    normalizer = noise(streams_of[14], (SEQS, HEADS, HEAD_DIM), 0.3, 1.75, ((0, 128),), jnp.float32)
    stabilizer = jnp.clip(jax.random.uniform(streams_of[15], (SEQS, HEADS), jnp.float32, -2.0, 2.0) * block_scale(streams_of[15], (SEQS, HEADS), ((0, 128),), -0.4, 0.0), -2.0, 2.0)
    output_weight = noise(streams_of[16], (D_MEM, D), D_MEM ** -0.5, 0.1875, ((1, 128),))
    expert_ids_keys = jax.random.split(jax.random.fold_in(streams_of[17], 1), SEQS // SEQ_DEV)
    expert_ids_turns = jax.random.permutation(jax.random.fold_in(streams_of[17], 3), SEQS // SEQ_DEV)
    expert_ids = jax.vmap(lambda own, number: deal_out(jax.random.fold_in(streams_of[17], 2), own, number, SEQ_DEV, EXPERTS, TOP_K, CAP, 2))(expert_ids_keys, expert_ids_turns).reshape((SEQS, TOP_K))
    route_weights = jnp.clip(0.2 + 0.6 * jax.random.uniform(streams_of[18], (SEQS, TOP_K), jnp.float32) ** block_scale(streams_of[18], (SEQS, TOP_K), ((0, 128),), -0.2, 0.2), 0.2, 0.8)
    expert_gate = noise(streams_of[19], (EXPERTS, D, FF), D ** -0.5, 0.125, ((0, 128),))
    expert_up = noise(streams_of[20], (EXPERTS, D, FF), D ** -0.5, 0.125, ((0, 128),))
    expert_down = noise(streams_of[21], (EXPERTS, FF, D), FF ** -0.5, 0.25, ((0, 128),))
    shared_gate = noise(streams_of[22], (D, FF), D ** -0.5, 0.125)
    shared_up = noise(streams_of[23], (D, FF), D ** -0.5, 0.125)
    shared_down = noise(streams_of[24], (FF, D), FF ** -0.5, 0.25)
    return dict(tokens=tokens, premix_gain=premix_gain, postmix_gain=postmix_gain, prefeed_gain=prefeed_gain, postfeed_gain=postfeed_gain, query_weight=query_weight, key_weight=key_weight, value_weight=value_weight, outgate_weight=outgate_weight, ingate_weight=ingate_weight, forget_weight=forget_weight, ingate_bias=ingate_bias, forget_bias=forget_bias, memory_state=memory_state, normalizer=normalizer, stabilizer=stabilizer, output_weight=output_weight, expert_ids=expert_ids, route_weights=route_weights, expert_gate=expert_gate, expert_up=expert_up, expert_down=expert_down, shared_gate=shared_gate, shared_up=shared_up, shared_down=shared_down)


epsilon = 1e-06

def rms_scale(values, gain_row):
    return values * lax.rsqrt(lax.optimization_barrier(jnp.mean(values * values, axis=-1, keepdims=True)) + epsilon) * gain_row

def rounded(values):
    return lax.optimization_barrier(values.astype(jnp.bfloat16))

def memory_step(queries, key_rows, value_rows, out_gate, input_pre, forget_pre, memory_state, normalizer, stabilizer):
    sequences = queries.shape[0]
    head_count = memory_state.shape[1]
    head_width = memory_state.shape[2]
    query_heads = queries.astype(jnp.float32).reshape(sequences, head_count, head_width)
    key_heads = key_rows.astype(jnp.float32).reshape(sequences, head_count, head_width) * head_width ** (-0.5)
    value_heads = value_rows.astype(jnp.float32).reshape(sequences, head_count, head_width)
    carried = jax.nn.log_sigmoid(forget_pre) + stabilizer
    next_stabilizer = jnp.maximum(carried, input_pre)
    keep_old = jnp.exp(carried - next_stabilizer)
    write_new = jnp.exp(input_pre - next_stabilizer)
    local_score = write_new * lax.optimization_barrier(jnp.sum(query_heads * key_heads, axis=-1))
    read_memory = jnp.einsum('shvk,shk->shv', memory_state, query_heads, precision=lax.Precision.HIGHEST)
    numerator = keep_old[..., None] * read_memory + local_score[..., None] * value_heads
    denominator = keep_old * lax.optimization_barrier(jnp.sum(normalizer * query_heads, axis=-1)) + local_score
    memory_read = numerator / jnp.maximum(jnp.abs(denominator), 1.0)[..., None]
    gated_out = (jax.nn.sigmoid(out_gate.astype(jnp.float32)) * memory_read.reshape(sequences, head_count * head_width)).astype(jnp.bfloat16)
    next_memory = keep_old[..., None, None] * memory_state + write_new[..., None, None] * value_heads[..., :, None] * key_heads[..., None, :]
    next_normalizer = keep_old[..., None] * normalizer + write_new[..., None] * key_heads
    return (gated_out, next_memory, next_normalizer, next_stabilizer)

def expert_rows(row_block, gate_weight, up_weight, down_weight):
    gate_values = jnp.dot(row_block, gate_weight, preferred_element_type=jnp.float32)
    up_values = jnp.dot(row_block, up_weight, preferred_element_type=jnp.float32)
    inner_rows = (jax.nn.silu(gate_values) * up_values).astype(jnp.bfloat16)
    return jnp.dot(inner_rows, down_weight, preferred_element_type=jnp.float32)

def reference(tokens, premix_gain, postmix_gain, prefeed_gain, postfeed_gain, query_weight, key_weight, value_weight, outgate_weight, ingate_weight, forget_weight, ingate_bias, forget_bias, memory_state, normalizer, stabilizer, output_weight, expert_ids, route_weights, expert_gate, expert_up, expert_down, shared_gate, shared_up, shared_down):
    residual = tokens.astype(jnp.float32)
    normed = rms_scale(residual, premix_gain).astype(jnp.bfloat16)
    queries = rounded(jnp.dot(normed, query_weight, preferred_element_type=jnp.float32))
    key_rows = rounded(jnp.dot(normed, key_weight, preferred_element_type=jnp.float32))
    value_rows = rounded(jnp.dot(normed, value_weight, preferred_element_type=jnp.float32))
    out_gate = rounded(jnp.dot(normed, outgate_weight, preferred_element_type=jnp.float32))
    input_pre = jnp.dot(normed, ingate_weight, preferred_element_type=jnp.float32) + ingate_bias
    forget_pre = jnp.dot(normed, forget_weight, preferred_element_type=jnp.float32) + forget_bias
    gated_out, next_memory, next_normalizer, next_stabilizer = memory_step(queries, key_rows, value_rows, out_gate, input_pre, forget_pre, memory_state, normalizer, stabilizer)
    mixed = rounded(jnp.dot(gated_out, output_weight, preferred_element_type=jnp.float32))
    after_mix = rounded(residual + rms_scale(mixed.astype(jnp.float32), postmix_gain))
    after_float = after_mix.astype(jnp.float32)
    expert_input = rms_scale(after_float, prefeed_gain).astype(jnp.bfloat16)
    flat_ids = expert_ids.reshape(-1).astype(jnp.int32)
    one_hot = (flat_ids[:, None] == jnp.arange(EXPERTS, dtype=jnp.int32)[None, :]).astype(jnp.int32)
    earlier = jnp.cumsum(one_hot, axis=0) - one_hot
    slot_ids = lax.optimization_barrier(jnp.sum(earlier * one_hot, axis=1)).astype(jnp.int32)
    token_index = (jnp.arange(SEQS * TOP_K, dtype=jnp.int32) // TOP_K).astype(jnp.int32)
    slot_table = jnp.zeros((EXPERTS, N_EP * CAP), jnp.int32).at[flat_ids, slot_ids].set(token_index)

    def one_expert(inputs):
        rows_index, gate_weight, up_weight, down_weight = inputs
        return expert_rows(expert_input[rows_index], gate_weight, up_weight, down_weight).astype(jnp.bfloat16)
    outputs = lax.map(one_expert, (slot_table, expert_gate, expert_up, expert_down))
    picked = outputs[flat_ids, slot_ids].astype(jnp.float32).reshape(SEQS, TOP_K, D)
    routed = lax.optimization_barrier(jnp.sum(picked * route_weights[:, :, None], axis=1))
    shared_out = expert_rows(expert_input, shared_gate, shared_up, shared_down)
    next_tokens = (after_float + rms_scale(routed + shared_out, postfeed_gain)).astype(jnp.bfloat16)
    return (next_tokens, next_memory, next_normalizer, next_stabilizer)
```

```python
import jax
import jax.numpy as jnp
from jax import lax
from jax.experimental import pallas as pl
from jax.experimental.pallas import tpu as pltpu
from jax.sharding import PartitionSpec as P

MESH = pl.DeviceIdType.MESH
epsilon = 1e-06
f32, bf16 = jnp.float32, jnp.bfloat16
N = 128


def rms_scale(values, gain_row):
    return (
        values * lax.rsqrt(jnp.mean(values * values, axis=-1, keepdims=True) + epsilon) * gain_row
    )


def dot(a, b):
    return jnp.dot(a, b, preferred_element_type=f32)


def dot_nt(a, b):
    return lax.dot_general(a, b, (((1,), (1,)), ((), ())), preferred_element_type=f32)


def rows(ref, at, count, step=8):
    return ref.at[pl.ds(pl.multiple_of(at, step), count)]


def spread(offsets):
    groups = {}
    for k, o in enumerate(sorted(offsets, key=lambda o: (o * 37) % 128)):
        c, x, y, z = o % 2, (o // 2) % 4, (o // 8) % 4, o // 32
        first = next((i, v) for i, v in ((2, x), (1, y), (0, z), (3, c)) if v)
        groups.setdefault(first, []).append((z, y, x, c))
    order, lists = [], list(groups.values())
    while any(lists):
        for entries in lists:
            if entries:
                order.append(entries.pop())
    return order


ALL = spread(range(1, N))


def mega(
    tok, g_pre, g_post, g_feed, g_out, wq, wk, wv, wo, wi, wf, b_in, b_fg, mem_hbm, nrm, stab, owt,
    ids, rw, eg_hbm, eu_hbm, ed_hbm, sg_hbm, su_hbm, sd_hbm,
    nt_out, nn_out, ns_out, keep_out, wv_out, k_out,
    mem, memb, eg, eu, ed, sg, su, sd,
    nb, wbuf, tok_a, w_a, out_b, recv_b, ow_a, g_a, out_c, recv_c, hsel, hwgt, d_out, d_in, u_in,
    hid, e_out, e_in, res,
    sem_l, sem_s, sem_r,
):
    me = lax.axis_index("ep")
    c, x, y, z = lax.rem(me, 2), lax.rem(lax.div(me, 2), 4), lax.rem(lax.div(me, 8), 4), lax.div(me, 32)
    xs = [lax.rem(x + d, 4) for d in range(4)]
    ys = [lax.rem(y + d, 4) for d in range(4)]
    zs = [lax.rem(z + d, 4) for d in range(4)]
    cs = [c, 1 - c]

    def dev(dz, dy, dx, dc):
        return zs[dz] * 32 + ys[dy] * 8 + xs[dx] * 2 + cs[dc]

    def send(src, dst, k, target):
        pltpu.make_async_remote_copy(
            src, dst, sem_s.at[k], sem_r.at[k], device_id=(target,), device_id_type=MESH
        ).start()

    def arrived(ref, k):
        pltpu.make_async_copy(ref, ref, sem_r.at[k]).wait()

    def sent(ref, k):
        pltpu.make_async_copy(ref, ref, sem_s.at[k]).wait()

    loads = [
        pltpu.make_async_copy(a, b, sem_l.at[k])
        for k, (a, b) in enumerate(
            (
                (mem_hbm, mem),
                (sg_hbm, sg),
                (su_hbm, su),
                (sd_hbm, sd),
                (eg_hbm, eg),
                (eu_hbm, eu),
                (ed_hbm, ed),
            )
        )
    ]
    loads[0].start()

    plane = [(0, dy, dx, 0) for dy in range(4) for dx in range(4) if dy or dx]
    zline = [(dz, 0, 0, 0) for dz in (1, 2, 3)]
    barrier = pltpu.get_barrier_semaphore()
    for o in plane + zline + [(0, 0, 0, 1)]:
        pl.semaphore_signal(barrier, inc=1, device_id=(dev(*o),), device_id_type=MESH)
    for load in loads[1:]:
        load.start()

    residual = tok[...].astype(f32)
    normed = rms_scale(residual, g_pre[...]).astype(bf16)
    for k in range(4):
        nb[8 * k : 8 * k + 8, :] = normed[:, 512 * k : 512 * k + 512]
    for j, w in enumerate((wq, wk, wv, wo)):
        wbuf[32 * j : 32 * j + 16, :] = w[:, :512]
        wbuf[32 * j + 16 : 32 * j + 32, :] = w[:, 512:]

    half = lax.div(y, 2)
    gi = half * 4 + x
    slot_a = (gi * 4 + z) * 8
    tok_a[pl.ds(pl.multiple_of(slot_a, 8), 8), :] = nb[pl.ds(pl.multiple_of(z * 8, 8), 8), :]
    at_plane = (y * 4 + x) * 2 + c
    w_a[pl.ds(pl.multiple_of(at_plane * 16, 16), 16), :] = wbuf[
        pl.ds(pl.multiple_of(gi * 16, 16), 16), :
    ]
    pl.semaphore_wait(barrier, 19)

    for dz in (1, 2, 3):
        send(rows(nb, zs[dz] * 8, 8), rows(tok_a, slot_a, 8), 0, dev(dz, 0, 0, 0))
    for _, dy, dx, _ in [o for o in ALL if o[0] == 0 and o[3] == 0]:
        chunk = lax.div(ys[dy], 2) * 4 + xs[dx]
        send(
            rows(wbuf, chunk * 16, 16, 16),
            rows(w_a, at_plane * 16, 16, 16),
            1,
            dev(0, dy, dx, 0),
        )
    arrived(tok_a.at[pl.ds(0, 24)], 0)
    group = [(dy, dx) for dx in (1, 3, 2, 0) for dy in (0, 2) if dx or dy]
    for dy, dx in group:
        send(rows(tok_a, gi * 32, 32, 32), rows(tok_a, gi * 32, 32, 32), 2, dev(0, dy, dx, 0))
    arrived(w_a.at[pl.ds(0, 240)], 1)
    for p in range(16):
        at = (2 * p + c) * 16
        send(rows(w_a, at, 16, 16), rows(w_a, at, 16, 16), 3, dev(0, 0, 0, 1))

    input_pre = dot(normed, wi[...]) + b_in[...]
    forget_pre = dot(normed, wf[...]) + b_fg[...]
    log_sig = jnp.minimum(forget_pre, 0.0) - jnp.log1p(jnp.exp(-jnp.abs(forget_pre)))
    carried = log_sig + stab[...]
    next_stab = jnp.maximum(carried, input_pre)
    keep_old = jnp.exp(carried - next_stab)
    write_new = jnp.exp(input_pre - next_stab)
    ns_out[...] = next_stab
    loads[0].wait()

    def convert(s, _):
        for h in range(8):
            memb[h, pl.ds(pl.multiple_of(s * 128, 128), 128), :] = mem[s, h].astype(bf16)
        return 0

    lax.fori_loop(0, 8, convert, 0)

    arrived(tok_a.at[pl.ds(0, 224)], 2)
    arrived(w_a.at[pl.ds(0, 256)], 3)

    out_b[...] = dot(tok_a[...], w_a[...]).astype(bf16)
    slot_b = (z * 8 + gi) * 8
    recv_b[pl.ds(pl.multiple_of(slot_b, 8), 8), :] = out_b[pl.ds(pl.multiple_of(slot_a, 8), 8), :]
    for dz, dy, dx, dc in ALL:
        if dc == 0 and dy in (0, 2):
            at = ((lax.div(ys[dy], 2) * 4 + xs[dx]) * 4 + zs[dz]) * 8
            send(rows(out_b, at, 8), rows(recv_b, slot_b, 8), 4, dev(dz, dy, dx, 0))

    jx = lax.div(me, 16)
    at_ow = lax.rem(me, 16) * 16
    mine = x * 2 + c
    for dz in range(4):
        for dy in range(4):
            target = zs[dz] * 32 + ys[dy] * 8 + jx
            if dz == 0 and dy == 0:

                @pl.when(target == me)
                def _():
                    ow_a[pl.ds(pl.multiple_of(at_ow, 16), 16), :] = owt[...]

                @pl.when(target != me)
                def _():
                    send(owt, rows(ow_a, at_ow, 16, 16), 5, target)
            else:
                send(owt, rows(ow_a, at_ow, 16, 16), 5, target)

    lane = lax.broadcasted_iota(jnp.int32, (8, 1024), 1)
    lane_e, lane_s, lane_q = lane // 8, (lane // 4) % 2, lane % 4
    hit = jnp.zeros((8, 1024), f32)
    wgt = jnp.zeros((8, 1024), f32)
    for k in range(6):
        same = ids[:, k : k + 1] == lane_e
        hit = jnp.where(same, 1.0, hit)
        wgt = jnp.where(same, rw[:, k : k + 1], wgt)
    rank_rows, count = [], jnp.zeros((1, 1024), f32)
    for t in range(8):
        rank_rows.append(count)
        count = count + hit[t : t + 1]
    rank = jnp.concatenate(rank_rows, axis=0)
    sel = jnp.where(rank == lane_s.astype(f32), hit, 0.0)
    wsel = sel * wgt
    for q in range(4):
        ok = lane_q == q
        hsel[8 * q : 8 * q + 8, :] = jnp.where(ok, sel, 0.0)
        part = jnp.where(ok, wsel, 0.0)
        high = part.astype(bf16).astype(f32)
        hwgt[8 * q : 8 * q + 8, :] = high
        hwgt[32 + 8 * q : 40 + 8 * q, :] = part - high

    arrived(recv_b.at[pl.ds(0, 248)], 4)
    summed = []
    for j in range(8):
        total = recv_b[8 * j : 8 * j + 8, :].astype(f32)
        for k in range(1, 4):
            total = total + recv_b[64 * k + 8 * j : 64 * k + 8 * j + 8, :].astype(f32)
        summed.append(total.astype(bf16))

    def head(kind, h):
        return summed[kind * 2 + h // 4][:, 128 * (h % 4) : 128 * (h % 4) + 128]

    sub = lax.broadcasted_iota(jnp.int32, (8, 128), 0)
    for h in range(8):
        q_b = head(0, h)
        q = q_b.astype(f32)
        k = head(1, h).astype(f32) * (128 ** -0.5)
        v = head(2, h).astype(f32)
        o = head(3, h).astype(f32)
        keep, write = keep_old[:, h : h + 1], write_new[:, h : h + 1]
        wide = dot_nt(q_b, memb[h])
        read = jnp.zeros((8, 128), f32)
        for s in range(8):
            read = jnp.where(sub == s, wide[:, 128 * s : 128 * s + 128], read)
        n_h = nrm[:, h, :]
        score = write * jnp.sum(q * k, axis=-1, keepdims=True)
        den = keep * jnp.sum(n_h * q, axis=-1, keepdims=True) + score
        num = keep * read + score * v
        gated = jax.nn.sigmoid(o) * (num / jnp.maximum(jnp.abs(den), 1.0))
        g_a[pl.ds(pl.multiple_of(mine * 8, 8), 8), 128 * h : 128 * h + 128] = gated.astype(bf16)
        nn_out[:, h, :] = keep * n_h + write * k
        keep_out[:, h, :] = jnp.broadcast_to(keep, (8, 128))
        wv_out[:, h, :] = write * v
        k_out[:, h, :] = k

    line = [(dx, dc) for dx in (1, 3, 2, 0) for dc in (0, 1) if dx or dc]
    for dx, dc in line:
        send(rows(g_a, mine * 8, 8), rows(g_a, mine * 8, 8), 6, dev(0, 0, dx, dc))

    @pl.when(jx == mine)
    def _():
        arrived(ow_a.at[pl.ds(0, 240)], 5)

    @pl.when(jx != mine)
    def _():
        arrived(ow_a, 5)

    arrived(g_a.at[pl.ds(0, 56)], 6)
    out_c[...] = dot_nt(g_a[...], ow_a[...]).astype(bf16)
    recv_c[pl.ds(pl.multiple_of(mine * 8, 8), 8), :] = out_c[pl.ds(pl.multiple_of(mine * 8, 8), 8), :]
    for dx, dc in line:
        at = (xs[dx] * 2 + cs[dc]) * 8
        send(rows(out_c, at, 8), rows(recv_c, mine * 8, 8), 7, dev(0, 0, dx, dc))
    arrived(recv_c.at[pl.ds(0, 56)], 7)
    mixed = jnp.concatenate([recv_c[8 * p : 8 * p + 8, :].astype(f32) for p in range(8)], axis=1)
    after_mix = (residual + rms_scale(mixed, g_post[...])).astype(bf16).astype(f32)
    expert_input = rms_scale(after_mix, g_feed[...])

    quarters = jnp.concatenate([expert_input[:, 512 * q : 512 * q + 512] for q in range(4)], axis=0).astype(bf16)
    sel_t = jnp.transpose(hsel[...]).astype(bf16)
    d_out[...] = dot(sel_t, quarters).astype(bf16)
    for o in ALL:
        target = dev(*o)
        send(rows(d_out, target * 8, 8), rows(d_in, me * 8, 8), 8, target)
    d_in[pl.ds(pl.multiple_of(me * 8, 8), 8), :] = d_out[pl.ds(pl.multiple_of(me * 8, 8), 8), :]

    for load in loads[1:4]:
        load.wait()
    x_in = expert_input.astype(bf16)
    s_hid = (jax.nn.silu(dot(x_in, sg[...])) * dot(x_in, su[...])).astype(bf16)
    shared = dot(s_hid, sd[...])
    for load in loads[4:]:
        load.wait()

    arrived(d_in.at[pl.ds(0, 1016)], 8)
    r_i = lax.broadcasted_iota(jnp.int32, (256, 1024), 0)
    c_i = lax.broadcasted_iota(jnp.int32, (256, 1024), 1)
    for q in range(4):
        pick = jnp.where(c_i == 4 * r_i + q, 1.0, 0.0).astype(bf16)
        u_in[:, 512 * q : 512 * q + 512] = dot(pick, d_in[...]).astype(bf16)

    def up_proj(n, _):
        cols = pl.ds(pl.multiple_of(n * 256, 256), 256)
        gate = dot(u_in[...], eg[0, :, cols])
        up = dot(u_in[...], eu[0, :, cols])
        hid[:, cols] = (jax.nn.silu(gate) * up).astype(bf16)
        return 0

    lax.fori_loop(0, 2, up_proj, 0)

    def down_proj(q, _):
        cols = pl.ds(pl.multiple_of(q * 512, 512), 512)
        res[q] = dot(hid[...], ed[0, :, cols]).astype(bf16)
        return 0

    lax.fori_loop(0, 4, down_proj, 0)
    r_t = lax.broadcasted_iota(jnp.int32, (1024, 256), 0)
    c_t = lax.broadcasted_iota(jnp.int32, (1024, 256), 1)
    total = None
    for q in range(4):
        place = jnp.where(r_t == 4 * c_t + q, 1.0, 0.0).astype(bf16)
        part = dot(place, res[q])
        total = part if total is None else total + part
    e_out[...] = total.astype(bf16)
    for o in ALL:
        target = dev(*o)
        send(rows(e_out, target * 8, 8), rows(e_in, me * 8, 8), 9, target)
    e_in[pl.ds(pl.multiple_of(me * 8, 8), 8), :] = e_out[pl.ds(pl.multiple_of(me * 8, 8), 8), :]

    sent(nb.at[pl.ds(0, 24)], 0)
    sent(w_a.at[pl.ds(0, 240)], 1)
    sent(tok_a.at[pl.ds(0, 224)], 2)
    sent(w_a.at[pl.ds(0, 256)], 3)
    sent(recv_b.at[pl.ds(0, 248)], 4)

    @pl.when(jx == mine)
    def _():
        sent(ow_a.at[pl.ds(0, 240)], 5)

    @pl.when(jx != mine)
    def _():
        sent(ow_a, 5)

    sent(g_a.at[pl.ds(0, 56)], 6)
    sent(recv_c.at[pl.ds(0, 56)], 7)
    sent(d_in.at[pl.ds(0, 1016)], 8)

    arrived(e_in.at[pl.ds(0, 1016)], 9)
    comb = dot(hwgt[...].astype(bf16), e_in[...])
    comb = comb[:32] + comb[32:]
    routed = jnp.concatenate([comb[8 * q : 8 * q + 8] for q in range(4)], axis=1)
    nt_out[...] = (after_mix + rms_scale(routed + shared, g_out[...])).astype(bf16)
    sent(e_in.at[pl.ds(0, 1016)], 9)


def update(mem, keep, wv, k, out):
    columns = jnp.transpose(wv[0])
    for h in range(8):
        out[0, h] = keep[0, h : h + 1, :] * mem[0, h] + columns[:, h : h + 1] * k[0, h : h + 1, :]


def on_device(
    tokens, premix_gain, postmix_gain, prefeed_gain, postfeed_gain, query_weight, key_weight,
    value_weight, outgate_weight, ingate_weight, forget_weight, ingate_bias, forget_bias,
    memory_state, normalizer, stabilizer, output_weight, expert_ids, route_weights, expert_gate,
    expert_up, expert_down, shared_gate, shared_up, shared_down,
):
    vm, hbm = pl.BlockSpec(memory_space=pltpu.VMEM), pl.BlockSpec(memory_space=pl.ANY)
    sd = jax.ShapeDtypeStruct
    buf = pltpu.VMEM
    nt, nn, ns, keep, wv, k = pl.pallas_call(
        mega,
        out_shape=[
            sd((8, 2048), bf16),
            sd((8, 8, 128), f32),
            sd((8, 8), f32),
            sd((8, 8, 128), f32),
            sd((8, 8, 128), f32),
            sd((8, 8, 128), f32),
        ],
        in_specs=[vm] * 13 + [hbm] + [vm] * 5 + [hbm] * 6,
        out_specs=[vm] * 6,
        scratch_shapes=[
            buf((8, 8, 128, 128), f32),
            buf((8, 1024, 128), bf16),
            buf((1, 2048, 512), bf16),
            buf((1, 2048, 512), bf16),
            buf((1, 512, 2048), bf16),
            buf((2048, 512), bf16),
            buf((2048, 512), bf16),
            buf((512, 2048), bf16),
            buf((32, 512), bf16),
            buf((128, 512), bf16),
            buf((256, 512), bf16),
            buf((512, 512), bf16),
            buf((256, 512), bf16),
            buf((256, 512), bf16),
            buf((256, 1024), bf16),
            buf((64, 1024), bf16),
            buf((64, 256), bf16),
            buf((64, 256), bf16),
            buf((32, 1024), f32),
            buf((64, 1024), f32),
            buf((1024, 512), bf16),
            buf((1024, 512), bf16),
            buf((256, 2048), bf16),
            buf((256, 512), bf16),
            buf((1024, 512), bf16),
            buf((1024, 512), bf16),
            buf((4, 256, 512), bf16),
            pltpu.SemaphoreType.DMA((7,)),
            pltpu.SemaphoreType.DMA((10,)),
            pltpu.SemaphoreType.DMA((10,)),
        ],
        compiler_params=pltpu.CompilerParams(
            collective_id=0, has_side_effects=True, vmem_limit_bytes=58 * 2**20
        ),
    )(
        tokens,
        premix_gain.reshape(1, -1),
        postmix_gain.reshape(1, -1),
        prefeed_gain.reshape(1, -1),
        postfeed_gain.reshape(1, -1),
        query_weight,
        key_weight,
        value_weight,
        outgate_weight,
        ingate_weight,
        forget_weight,
        ingate_bias.reshape(1, -1),
        forget_bias.reshape(1, -1),
        memory_state,
        normalizer,
        stabilizer,
        output_weight.T,
        expert_ids,
        route_weights,
        expert_gate,
        expert_up,
        expert_down,
        shared_gate,
        shared_up,
        shared_down,
    )
    small = pl.BlockSpec((1, 8, 128), lambda s: (s, 0, 0))
    big = pl.BlockSpec((1, 8, 128, 128), lambda s: (s, 0, 0, 0))
    nm = pl.pallas_call(
        update,
        grid=(8,),
        in_specs=[big, small, small, small],
        out_specs=big,
        out_shape=sd((8, 8, 128, 128), f32),
        compiler_params=pltpu.CompilerParams(dimension_semantics=("arbitrary",)),
    )(memory_state, keep, wv, k)
    return (nt, nm, nn, ns)


def solution(mesh):
    e2, e3, e4 = P("ep", None), P("ep", None, None), P("ep", None, None, None)
    in_specs = (
        e2, P(), P(), P(), P(), e2, e2, e2, e2, P(), P(), P(), P(), e4, e3, e2, P(None, "ep"),
        e2, e2, e3, e3, e3, P(), P(), P(),
    )
    return jax.shard_map(
        on_device, mesh=mesh, in_specs=in_specs, out_specs=(e2, e4, e3, e2), check_vma=False
    )
```

```python
import jax
import jax.numpy as jnp
from jax import lax
from jax.experimental import pallas as pl
from jax.experimental.pallas import tpu as pltpu
from jax.sharding import PartitionSpec as P

MESH = pl.DeviceIdType.MESH
epsilon = 1e-06
f32, bf16 = jnp.float32, jnp.bfloat16
N = 128
SEQ_STEP = 2


def rms_scale(values, gain_row):
    return (
        values * lax.rsqrt(jnp.mean(values * values, axis=-1, keepdims=True) + epsilon) * gain_row
    )


def dot(a, b):
    return jnp.dot(a, b, preferred_element_type=f32)


def dot_nt(a, b):
    return lax.dot_general(a, b, (((1,), (1,)), ((), ())), preferred_element_type=f32)


def rows(ref, at, count, step=8):
    return ref.at[pl.ds(pl.multiple_of(at, step), count)]


def spread(offsets):
    groups = {}
    for k, o in enumerate(sorted(offsets, key=lambda o: (o * 37) % 128)):
        c, x, y, z = o % 2, (o // 2) % 4, (o // 8) % 4, o // 32
        first = next((i, v) for i, v in ((2, x), (1, y), (0, z), (3, c)) if v)
        groups.setdefault(first, []).append((z, y, x, c))
    order, lists = [], list(groups.values())
    while any(lists):
        for entries in lists:
            if entries:
                order.append(entries.pop())
    return order


ALL = spread(range(1, N))
CHUNKS = ((0, 2), (1, 3))


def mega(
    tok, g_pre, g_post, g_feed, g_out, wq, wk, wv, wo, wi, wf, b_in, b_fg, mem_hbm, nrm, stab, owt,
    ids, rw, eg_hbm, eu_hbm, ed_hbm, sg_hbm, su_hbm, sd_hbm,
    nt_out, nn_out, ns_out, keep_out, wv_out, k_out,
    mem, memb, eg, eu, ed, sg, su, sd,
    nb, wbuf, tok_a, w_a, out_b, recv_b, ow_a, g_a, out_c, recv_c, hsel, hwgt, d_out, d_in, u_in,
    hid, e_out, e_in, res,
    sem_l, sem_s, sem_r,
):
    me = lax.axis_index("ep")
    c, x, y, z = lax.rem(me, 2), lax.rem(lax.div(me, 2), 4), lax.rem(lax.div(me, 8), 4), lax.div(me, 32)
    xs = [lax.rem(x + d, 4) for d in range(4)]
    ys = [lax.rem(y + d, 4) for d in range(4)]
    zs = [lax.rem(z + d, 4) for d in range(4)]
    cs = [c, 1 - c]

    def dev(dz, dy, dx, dc):
        return zs[dz] * 32 + ys[dy] * 8 + xs[dx] * 2 + cs[dc]

    def send(src, dst, k, target):
        pltpu.make_async_remote_copy(
            src, dst, sem_s.at[k], sem_r.at[k], device_id=(target,), device_id_type=MESH
        ).start()

    def arrived(ref, k):
        pltpu.make_async_copy(ref, ref, sem_r.at[k]).wait()

    def sent(ref, k):
        pltpu.make_async_copy(ref, ref, sem_s.at[k]).wait()

    loads = [
        pltpu.make_async_copy(a, b, sem_l.at[k])
        for k, (a, b) in enumerate(
            (
                (mem_hbm, mem),
                (sg_hbm, sg),
                (su_hbm, su),
                (sd_hbm, sd),
                (eg_hbm, eg),
                (eu_hbm, eu),
                (ed_hbm, ed),
            )
        )
    ]
    loads[0].start()

    plane = [(0, dy, dx, 0) for dy in range(4) for dx in range(4) if dy or dx]
    zline = [(dz, 0, 0, 0) for dz in (1, 2, 3)]
    barrier = pltpu.get_barrier_semaphore()
    for o in plane + zline + [(0, 0, 0, 1)]:
        pl.semaphore_signal(barrier, inc=1, device_id=(dev(*o),), device_id_type=MESH)
    for load in loads[1:]:
        load.start()

    residual = tok[...].astype(f32)
    normed = rms_scale(residual, g_pre[...]).astype(bf16)
    for k in range(4):
        nb[8 * k : 8 * k + 8, :] = normed[:, 512 * k : 512 * k + 512]
    for j, w in enumerate((wq, wk, wv, wo)):
        wbuf[32 * j : 32 * j + 16, :] = w[:, :512]
        wbuf[32 * j + 16 : 32 * j + 32, :] = w[:, 512:]

    half = lax.div(y, 2)
    gi = half * 4 + x
    slot_a = (gi * 4 + z) * 8
    tok_a[pl.ds(pl.multiple_of(slot_a, 8), 8), :] = nb[pl.ds(pl.multiple_of(z * 8, 8), 8), :]
    at_plane = (y * 4 + x) * 2 + c
    w_a[pl.ds(pl.multiple_of(at_plane * 16, 16), 16), :] = wbuf[
        pl.ds(pl.multiple_of(gi * 16, 16), 16), :
    ]
    pl.semaphore_wait(barrier, 19)

    for dz in (1, 2, 3):
        send(rows(nb, zs[dz] * 8, 8), rows(tok_a, slot_a, 8), 0, dev(dz, 0, 0, 0))
    for _, dy, dx, _ in [o for o in ALL if o[0] == 0 and o[3] == 0]:
        chunk = lax.div(ys[dy], 2) * 4 + xs[dx]
        send(
            rows(wbuf, chunk * 16, 16, 16),
            rows(w_a, at_plane * 16, 16, 16),
            1,
            dev(0, dy, dx, 0),
        )
    arrived(tok_a.at[pl.ds(0, 24)], 0)
    group = [(dy, dx) for dx in (1, 3, 2, 0) for dy in (0, 2) if dx or dy]
    for dy, dx in group:
        send(rows(tok_a, gi * 32, 32, 32), rows(tok_a, gi * 32, 32, 32), 2, dev(0, dy, dx, 0))
    arrived(w_a.at[pl.ds(0, 240)], 1)
    for p in range(16):
        at = (2 * p + c) * 16
        send(rows(w_a, at, 16, 16), rows(w_a, at, 16, 16), 3, dev(0, 0, 0, 1))

    input_pre = dot_nt(normed, wi[...]) + b_in[...]
    forget_pre = dot_nt(normed, wf[...]) + b_fg[...]
    log_sig = jnp.minimum(forget_pre, 0.0) - jnp.log1p(jnp.exp(-jnp.abs(forget_pre)))
    carried = log_sig + stab[...]
    next_stab = jnp.maximum(carried, input_pre)
    keep_old = jnp.exp(carried - next_stab)
    write_new = jnp.exp(input_pre - next_stab)
    ns_out[...] = next_stab
    loads[0].wait()

    def convert(s, _):
        for h in range(8):
            memb[h, pl.ds(pl.multiple_of(s * 128, 128), 128), :] = mem[s, h].astype(bf16)
        return 0

    lax.fori_loop(0, 8, convert, 0)

    arrived(tok_a.at[pl.ds(0, 224)], 2)
    arrived(w_a.at[pl.ds(0, 256)], 3)

    out_b[...] = dot(tok_a[...], w_a[...]).astype(bf16)
    slot_b = (z * 8 + gi) * 8
    recv_b[pl.ds(pl.multiple_of(slot_b, 8), 8), :] = out_b[pl.ds(pl.multiple_of(slot_a, 8), 8), :]
    for dz, dy, dx, dc in ALL:
        if dc == 0 and dy in (0, 2):
            at = ((lax.div(ys[dy], 2) * 4 + xs[dx]) * 4 + zs[dz]) * 8
            send(rows(out_b, at, 8), rows(recv_b, slot_b, 8), 4, dev(dz, dy, dx, 0))

    jx = lax.div(me, 16)
    jx_x, jx_c = lax.div(jx, 2), lax.rem(jx, 2)
    at_ow = lax.rem(me, 16) * 16
    mine = x * 2 + c
    jm = lax.rem(x + 8 - z - y, 4) * 2 + c
    for dz in range(4):
        for dy in range(4):
            target = zs[dz] * 32 + ys[dy] * 8 + lax.rem(jx_x + zs[dz] + ys[dy], 4) * 2 + jx_c
            if dz == 0 and dy == 0:

                @pl.when(target == me)
                def _():
                    ow_a[pl.ds(pl.multiple_of(at_ow, 16), 16), :] = owt[...]

                @pl.when(target != me)
                def _():
                    send(owt, rows(ow_a, at_ow, 16, 16), 5, target)
            else:
                send(owt, rows(ow_a, at_ow, 16, 16), 5, target)

    lane = lax.broadcasted_iota(jnp.int32, (8, 1024), 1)
    lane_e, lane_s, lane_q = lane // 8, (lane // 4) % 2, lane % 4
    hit = jnp.zeros((8, 1024), f32)
    wgt = jnp.zeros((8, 1024), f32)
    for k in range(6):
        same = ids[:, k : k + 1] == lane_e
        hit = jnp.where(same, 1.0, hit)
        wgt = jnp.where(same, rw[:, k : k + 1], wgt)
    rank_rows, count = [], jnp.zeros((1, 1024), f32)
    for t in range(8):
        rank_rows.append(count)
        count = count + hit[t : t + 1]
    rank = jnp.concatenate(rank_rows, axis=0)
    sel = jnp.where(rank == lane_s.astype(f32), hit, 0.0)
    wsel = sel * wgt
    for q in range(4):
        ok = lane_q == q
        hsel[8 * q : 8 * q + 8, :] = jnp.where(ok, sel, 0.0)
        part = jnp.where(ok, wsel, 0.0)
        high = part.astype(bf16).astype(f32)
        hwgt[8 * q : 8 * q + 8, :] = high
        hwgt[32 + 8 * q : 40 + 8 * q, :] = part - high

    arrived(recv_b.at[pl.ds(0, 248)], 4)
    summed = []
    for j in range(8):
        total = recv_b[8 * j : 8 * j + 8, :].astype(f32)
        for k in range(1, 4):
            total = total + recv_b[64 * k + 8 * j : 64 * k + 8 * j + 8, :].astype(f32)
        summed.append(total.astype(bf16))

    def head(kind, h):
        return summed[kind * 2 + h // 4][:, 128 * (h % 4) : 128 * (h % 4) + 128]

    sub = lax.broadcasted_iota(jnp.int32, (8, 128), 0)
    for h in range(8):
        q_b = head(0, h)
        q = q_b.astype(f32)
        k = head(1, h).astype(f32) * (128 ** -0.5)
        v = head(2, h).astype(f32)
        o = head(3, h).astype(f32)
        keep, write = keep_old[:, h : h + 1], write_new[:, h : h + 1]
        wide = dot_nt(q_b, memb[h])
        read = jnp.zeros((8, 128), f32)
        for s in range(8):
            read = jnp.where(sub == s, wide[:, 128 * s : 128 * s + 128], read)
        n_h = nrm[:, h, :]
        score = write * jnp.sum(q * k, axis=-1, keepdims=True)
        den = keep * jnp.sum(n_h * q, axis=-1, keepdims=True) + score
        num = keep * read + score * v
        gated = jax.nn.sigmoid(o) * (num / jnp.maximum(jnp.abs(den), 1.0))
        g_a[pl.ds(pl.multiple_of(mine * 8, 8), 8), 128 * h : 128 * h + 128] = gated.astype(bf16)
        nn_out[:, h, :] = keep * n_h + write * k
        keep_out[:, h, :] = jnp.broadcast_to(keep, (8, 128))
        wv_out[:, h, :] = write * v
        k_out[:, h, :] = k

    line = [(dx, dc) for dx in (1, 3, 2, 0) for dc in (0, 1) if dx or dc]
    for dx, dc in line:
        send(rows(g_a, mine * 8, 8), rows(g_a, mine * 8, 8), 6, dev(0, 0, dx, dc))

    @pl.when(jx == jm)
    def _():
        arrived(ow_a.at[pl.ds(0, 240)], 5)

    @pl.when(jx != jm)
    def _():
        arrived(ow_a, 5)

    arrived(g_a.at[pl.ds(0, 56)], 6)
    out_c[...] = dot_nt(g_a[...], ow_a[...]).astype(bf16)
    recv_c[pl.ds(pl.multiple_of(jm * 8, 8), 8), :] = out_c[pl.ds(pl.multiple_of(mine * 8, 8), 8), :]
    for dx, dc in line:
        at = (xs[dx] * 2 + cs[dc]) * 8
        send(rows(out_c, at, 8), rows(recv_c, jm * 8, 8), 7, dev(0, 0, dx, dc))
    arrived(recv_c.at[pl.ds(0, 56)], 7)
    mixed = jnp.concatenate([recv_c[8 * p : 8 * p + 8, :].astype(f32) for p in range(8)], axis=1)
    after_mix = (residual + rms_scale(mixed, g_post[...])).astype(bf16).astype(f32)
    expert_input = rms_scale(after_mix, g_feed[...])

    quarters = jnp.concatenate([expert_input[:, 512 * q : 512 * q + 512] for q in range(4)], axis=0).astype(bf16)
    sel_t = jnp.transpose(hsel[...]).astype(bf16)
    d_out[...] = dot(sel_t, quarters).astype(bf16)
    for n, planes in enumerate(CHUNKS):
        for o in ALL:
            if o[0] in planes:
                target = dev(*o)
                send(rows(d_out, target * 8, 8), rows(d_in, me * 8, 8), 8 + n, target)
    d_in[pl.ds(pl.multiple_of(me * 8, 8), 8), :] = d_out[pl.ds(pl.multiple_of(me * 8, 8), 8), :]

    for load in loads[1:4]:
        load.wait()
    x_in = expert_input.astype(bf16)
    s_hid = (jax.nn.silu(dot(x_in, sg[...])) * dot(x_in, su[...])).astype(bf16)
    shared = dot(s_hid, sd[...])
    for load in loads[4:]:
        load.wait()

    r_i = lax.broadcasted_iota(jnp.int32, (64, 256), 0)
    c_i = lax.broadcasted_iota(jnp.int32, (64, 256), 1)
    r_t = lax.broadcasted_iota(jnp.int32, (256, 64), 0)
    c_t = lax.broadcasted_iota(jnp.int32, (256, 64), 1)
    picks = [jnp.where(c_i == 4 * r_i + q, 1.0, 0.0).astype(bf16) for q in range(4)]
    places = [jnp.where(r_t == 4 * c_t + q, 1.0, 0.0).astype(bf16) for q in range(4)]
    for n, planes in enumerate(CHUNKS):
        arrived(d_in.at[pl.ds(0, 256 * len(planes) - (8 if 0 in planes else 0))], 8 + n)
        size = 64 * len(planes)
        for i, dz in enumerate(planes):
            block = d_in[pl.ds(pl.multiple_of(zs[-dz % 4] * 256, 256), 256), :]
            for q in range(4):
                u_in[64 * i : 64 * i + 64, 512 * q : 512 * q + 512] = dot(picks[q], block).astype(bf16)

        def up_proj(k, _):
            cols = pl.ds(pl.multiple_of(k * 256, 256), 256)
            gate = dot(u_in[:size], eg[0, :, cols])
            up = dot(u_in[:size], eu[0, :, cols])
            hid[:size, cols] = (jax.nn.silu(gate) * up).astype(bf16)
            return 0

        lax.fori_loop(0, 2, up_proj, 0)

        def down_proj(q, _):
            cols = pl.ds(pl.multiple_of(q * 512, 512), 512)
            res[q, :size] = dot(hid[:size], ed[0, :, cols]).astype(bf16)
            return 0

        lax.fori_loop(0, 4, down_proj, 0)
        for i, dz in enumerate(planes):
            total = None
            for q in range(4):
                part = dot(places[q], res[q, 64 * i : 64 * i + 64])
                total = part if total is None else total + part
            e_out[pl.ds(pl.multiple_of(zs[-dz % 4] * 256, 256), 256), :] = total.astype(bf16)
        for o in ALL:
            if -o[0] % 4 in planes:
                target = dev(*o)
                send(rows(e_out, target * 8, 8), rows(e_in, me * 8, 8), 8 + len(CHUNKS), target)
    e_in[pl.ds(pl.multiple_of(me * 8, 8), 8), :] = e_out[pl.ds(pl.multiple_of(me * 8, 8), 8), :]

    sent(nb.at[pl.ds(0, 24)], 0)
    sent(w_a.at[pl.ds(0, 240)], 1)
    sent(tok_a.at[pl.ds(0, 224)], 2)
    sent(w_a.at[pl.ds(0, 256)], 3)
    sent(recv_b.at[pl.ds(0, 248)], 4)

    @pl.when(jx == jm)
    def _():
        sent(ow_a.at[pl.ds(0, 240)], 5)

    @pl.when(jx != jm)
    def _():
        sent(ow_a, 5)

    sent(g_a.at[pl.ds(0, 56)], 6)
    sent(recv_c.at[pl.ds(0, 56)], 7)
    for n, planes in enumerate(CHUNKS):
        sent(d_in.at[pl.ds(0, 256 * len(planes) - (8 if 0 in planes else 0))], 8 + n)

    arrived(e_in.at[pl.ds(0, 1016)], 8 + len(CHUNKS))
    comb = dot(hwgt[...].astype(bf16), e_in[...])
    comb = comb[:32] + comb[32:]
    routed = jnp.concatenate([comb[8 * q : 8 * q + 8] for q in range(4)], axis=1)
    nt_out[...] = (after_mix + rms_scale(routed + shared, g_out[...])).astype(bf16)
    sent(e_in.at[pl.ds(0, 1016)], 8 + len(CHUNKS))


def update(mem, keep, wv, k, nt, nn, ns, out, nt_out, nn_out, ns_out):
    step = pl.program_id(0)

    @pl.when(step == 0)
    def _():
        nt_out[...] = nt[...]
        nn_out[...] = nn[...]
        ns_out[...] = ns[...]

    for i in range(SEQ_STEP):
        s = step * SEQ_STEP + i
        columns = jnp.transpose(wv[s])
        kept, keys = keep[s], k[s]
        for h in range(8):
            out[i, h] = kept[h : h + 1, :] * mem[i, h] + columns[:, h : h + 1] * keys[h : h + 1, :]


def on_device(
    tokens, premix_gain, postmix_gain, prefeed_gain, postfeed_gain, query_weight, key_weight,
    value_weight, outgate_weight, ingate_weight, forget_weight, ingate_bias, forget_bias,
    memory_state, normalizer, stabilizer, output_weight, expert_ids, route_weights, expert_gate,
    expert_up, expert_down, shared_gate, shared_up, shared_down,
):
    vm, hbm = pl.BlockSpec(memory_space=pltpu.VMEM), pl.BlockSpec(memory_space=pl.ANY)
    sd = jax.ShapeDtypeStruct
    buf = pltpu.VMEM
    nt, nn, ns, keep, wv, k = pl.pallas_call(
        mega,
        out_shape=[
            sd((8, 2048), bf16),
            sd((8, 8, 128), f32),
            sd((8, 8), f32),
            sd((8, 8, 128), f32),
            sd((8, 8, 128), f32),
            sd((8, 8, 128), f32),
        ],
        in_specs=[vm] * 13 + [hbm] + [vm] * 5 + [hbm] * 6,
        out_specs=[vm] * 6,
        scratch_shapes=[
            buf((8, 8, 128, 128), f32),
            buf((8, 1024, 128), bf16),
            buf((1, 2048, 512), bf16),
            buf((1, 2048, 512), bf16),
            buf((1, 512, 2048), bf16),
            buf((2048, 512), bf16),
            buf((2048, 512), bf16),
            buf((512, 2048), bf16),
            buf((32, 512), bf16),
            buf((128, 512), bf16),
            buf((256, 512), bf16),
            buf((512, 512), bf16),
            buf((256, 512), bf16),
            buf((256, 512), bf16),
            buf((256, 1024), bf16),
            buf((64, 1024), bf16),
            buf((64, 256), bf16),
            buf((64, 256), bf16),
            buf((32, 1024), f32),
            buf((64, 1024), f32),
            buf((1024, 512), bf16),
            buf((1024, 512), bf16),
            buf((256, 2048), bf16),
            buf((256, 512), bf16),
            buf((1024, 512), bf16),
            buf((1024, 512), bf16),
            buf((4, 256, 512), bf16),
            pltpu.SemaphoreType.DMA((7,)),
            pltpu.SemaphoreType.DMA((9 + len(CHUNKS),)),
            pltpu.SemaphoreType.DMA((9 + len(CHUNKS),)),
        ],
        compiler_params=pltpu.CompilerParams(
            collective_id=0, has_side_effects=True, vmem_limit_bytes=58 * 2**20
        ),
    )(
        tokens,
        premix_gain.reshape(1, -1),
        postmix_gain.reshape(1, -1),
        prefeed_gain.reshape(1, -1),
        postfeed_gain.reshape(1, -1),
        query_weight,
        key_weight,
        value_weight,
        outgate_weight,
        ingate_weight.T,
        forget_weight.T,
        ingate_bias.reshape(1, -1),
        forget_bias.reshape(1, -1),
        memory_state,
        normalizer,
        stabilizer,
        output_weight.T,
        expert_ids,
        route_weights,
        expert_gate,
        expert_up,
        expert_down,
        shared_gate,
        shared_up,
        shared_down,
    )
    big = pl.BlockSpec((SEQ_STEP, 8, 128, 128), lambda s: (s, 0, 0, 0))
    nm, nt, nn, ns = pl.pallas_call(
        update,
        grid=(8 // SEQ_STEP,),
        in_specs=[big] + [vm] * 6,
        out_specs=[big] + [vm] * 3,
        out_shape=[sd((8, 8, 128, 128), f32), sd((8, 2048), bf16), sd((8, 8, 128), f32), sd((8, 8), f32)],
        compiler_params=pltpu.CompilerParams(dimension_semantics=("arbitrary",)),
    )(memory_state, keep, wv, k, nt, nn, ns)
    return (nt, nm, nn, ns)


def solution(mesh):
    e2, e3, e4 = P("ep", None), P("ep", None, None), P("ep", None, None, None)
    in_specs = (
        e2, P(), P(), P(), P(), e2, e2, e2, e2, P(), P(), P(), P(), e4, e3, e2, P(None, "ep"),
        e2, e2, e3, e3, e3, P(), P(), P(),
    )
    return jax.shard_map(
        on_device, mesh=mesh, in_specs=in_specs, out_specs=(e2, e4, e3, e2), check_vma=False
    )
```

```python
import jax
import jax.numpy as jnp
from jax import lax
from jax.experimental import pallas as pl
from jax.experimental.pallas import tpu as pltpu
from jax.sharding import PartitionSpec as P

MESH = pl.DeviceIdType.MESH
epsilon = 1e-06
f32, bf16 = jnp.float32, jnp.bfloat16
N = 128


def rms_scale(values, gain_row):
    return (
        values * lax.rsqrt(jnp.mean(values * values, axis=-1, keepdims=True) + epsilon) * gain_row
    )


def dot(a, b):
    return jnp.dot(a, b, preferred_element_type=f32)


def dot_nt(a, b):
    return lax.dot_general(a, b, (((1,), (1,)), ((), ())), preferred_element_type=f32)


def rows(ref, at, count, step=8):
    return ref.at[pl.ds(pl.multiple_of(at, step), count)]


def spread(offsets):
    groups = {}
    for k, o in enumerate(sorted(offsets, key=lambda o: (o * 37) % 128)):
        c, x, y, z = o % 2, (o // 2) % 4, (o // 8) % 4, o // 32
        first = next((i, v) for i, v in ((2, x), (1, y), (0, z), (3, c)) if v)
        groups.setdefault(first, []).append((z, y, x, c))
    order, lists = [], list(groups.values())
    while any(lists):
        for entries in lists:
            if entries:
                order.append(entries.pop())
    return order


ALL = spread(range(1, N))
CHUNKS = ((0, 2), (1, 3))


def mega(
    tok, g_pre, g_post, g_feed, g_out, wq, wk, wv, wo, wi, wf, b_in, b_fg, mem_hbm, nrm, stab, owt,
    ids, rw, eg_hbm, eu_hbm, ed_hbm, sg_hbm, su_hbm, sd_hbm,
    nt_out, nn_out, ns_out, nm_out, mem, memb, eg, eu, ed, sg, su, sd,
    nb, wbuf, tok_a, w_a, out_b, recv_b, ow_a, g_a, out_c, recv_c, hsel, hwgt, d_out, d_in, u_in,
    hid, e_out, e_in, res, keep_b, wv_b, k_b,
    sem_l, sem_s, sem_r, sem_k,
):
    me = lax.axis_index("ep")
    c, x, y, z = lax.rem(me, 2), lax.rem(lax.div(me, 2), 4), lax.rem(lax.div(me, 8), 4), lax.div(me, 32)
    xs = [lax.rem(x + d, 4) for d in range(4)]
    ys = [lax.rem(y + d, 4) for d in range(4)]
    zs = [lax.rem(z + d, 4) for d in range(4)]
    cs = [c, 1 - c]

    def dev(dz, dy, dx, dc):
        return zs[dz] * 32 + ys[dy] * 8 + xs[dx] * 2 + cs[dc]

    def send(src, dst, k, target):
        pltpu.make_async_remote_copy(
            src, dst, sem_s.at[k], sem_r.at[k], device_id=(target,), device_id_type=MESH
        ).start()

    def arrived(ref, k):
        pltpu.make_async_copy(ref, ref, sem_r.at[k]).wait()

    def sent(ref, k):
        pltpu.make_async_copy(ref, ref, sem_s.at[k]).wait()

    loads = [
        pltpu.make_async_copy(a, b, sem_l.at[k])
        for k, (a, b) in enumerate(
            (
                (mem_hbm, mem),
                (sg_hbm, sg),
                (su_hbm, su),
                (sd_hbm, sd),
                (eg_hbm, eg),
                (eu_hbm, eu),
                (ed_hbm, ed),
            )
        )
    ]
    loads[0].start()

    plane = [(0, dy, dx, 0) for dy in range(4) for dx in range(4) if dy or dx]
    zline = [(dz, 0, 0, 0) for dz in (1, 2, 3)]
    barrier = pltpu.get_barrier_semaphore()
    for o in plane + zline + [(0, 0, 0, 1)]:
        pl.semaphore_signal(barrier, inc=1, device_id=(dev(*o),), device_id_type=MESH)
    for load in loads[1:]:
        load.start()

    residual = tok[...].astype(f32)
    normed = rms_scale(residual, g_pre[...]).astype(bf16)
    for k in range(4):
        nb[8 * k : 8 * k + 8, :] = normed[:, 512 * k : 512 * k + 512]
    for j, w in enumerate((wq, wk, wv, wo)):
        wbuf[32 * j : 32 * j + 16, :] = w[:, :512]
        wbuf[32 * j + 16 : 32 * j + 32, :] = w[:, 512:]

    half = lax.div(y, 2)
    gi = half * 4 + x
    slot_a = (gi * 4 + z) * 8
    tok_a[pl.ds(pl.multiple_of(slot_a, 8), 8), :] = nb[pl.ds(pl.multiple_of(z * 8, 8), 8), :]
    at_plane = (y * 4 + x) * 2 + c
    w_a[pl.ds(pl.multiple_of(at_plane * 16, 16), 16), :] = wbuf[
        pl.ds(pl.multiple_of(gi * 16, 16), 16), :
    ]
    pl.semaphore_wait(barrier, 19)

    for dz in (1, 2, 3):
        send(rows(nb, zs[dz] * 8, 8), rows(tok_a, slot_a, 8), 0, dev(dz, 0, 0, 0))
    for _, dy, dx, _ in [o for o in ALL if o[0] == 0 and o[3] == 0]:
        chunk = lax.div(ys[dy], 2) * 4 + xs[dx]
        send(
            rows(wbuf, chunk * 16, 16, 16),
            rows(w_a, at_plane * 16, 16, 16),
            1,
            dev(0, dy, dx, 0),
        )
    arrived(tok_a.at[pl.ds(0, 24)], 0)
    group = [(dy, dx) for dx in (1, 3, 2, 0) for dy in (0, 2) if dx or dy]
    for dy, dx in group:
        send(rows(tok_a, gi * 32, 32, 32), rows(tok_a, gi * 32, 32, 32), 2, dev(0, dy, dx, 0))
    pl.semaphore_signal(sem_k, inc=1, device_id=(dev(0, 0, 0, 1),), device_id_type=MESH)
    arrived(w_a.at[pl.ds(0, 240)], 1)
    for p in range(16):
        at = (2 * p + c) * 16
        send(rows(w_a, at, 16, 16), rows(w_a, at, 16, 16), 3, dev(0, 0, 0, 1))

    pl.semaphore_wait(sem_k, 1)

    input_pre = dot_nt(normed, wi[...]) + b_in[...]
    forget_pre = dot_nt(normed, wf[...]) + b_fg[...]
    log_sig = jnp.minimum(forget_pre, 0.0) - jnp.log1p(jnp.exp(-jnp.abs(forget_pre)))
    carried = log_sig + stab[...]
    next_stab = jnp.maximum(carried, input_pre)
    keep_old = jnp.exp(carried - next_stab)
    write_new = jnp.exp(input_pre - next_stab)
    ns_out[...] = next_stab
    loads[0].wait()

    def convert(s, _):
        for h in range(8):
            memb[h, pl.ds(pl.multiple_of(s * 128, 128), 128), :] = mem[s, h].astype(bf16)
        return 0

    lax.fori_loop(0, 8, convert, 0)

    arrived(tok_a.at[pl.ds(0, 224)], 2)
    arrived(w_a.at[pl.ds(0, 256)], 3)

    out_b[...] = dot(tok_a[...], w_a[...]).astype(bf16)
    slot_b = (z * 8 + gi) * 8
    recv_b[pl.ds(pl.multiple_of(slot_b, 8), 8), :] = out_b[pl.ds(pl.multiple_of(slot_a, 8), 8), :]
    for dz, dy, dx, dc in ALL:
        if dc == 0 and dy in (0, 2):
            at = ((lax.div(ys[dy], 2) * 4 + xs[dx]) * 4 + zs[dz]) * 8
            send(rows(out_b, at, 8), rows(recv_b, slot_b, 8), 4, dev(dz, dy, dx, 0))

    jx = lax.div(me, 16)
    jx_x, jx_c = lax.div(jx, 2), lax.rem(jx, 2)
    at_ow = lax.rem(me, 16) * 16
    mine = x * 2 + c
    jm = lax.rem(x + 8 - 2 * c - z - y, 4) * 2 + c
    for dz in range(4):
        for dy in range(4):
            target = zs[dz] * 32 + ys[dy] * 8 + lax.rem(jx_x + 2 * jx_c + zs[dz] + ys[dy], 4) * 2 + jx_c
            if dz == 0 and dy == 0:

                @pl.when(target == me)
                def _():
                    ow_a[pl.ds(pl.multiple_of(at_ow, 16), 16), :] = owt[...]

                @pl.when(target != me)
                def _():
                    send(owt, rows(ow_a, at_ow, 16, 16), 5, target)
            else:
                send(owt, rows(ow_a, at_ow, 16, 16), 5, target)

    lane = lax.broadcasted_iota(jnp.int32, (8, 1024), 1)
    lane_e, lane_s, lane_q = lane // 8, (lane // 4) % 2, lane % 4
    hit = jnp.zeros((8, 1024), f32)
    wgt = jnp.zeros((8, 1024), f32)
    for k in range(6):
        same = ids[:, k : k + 1] == lane_e
        hit = jnp.where(same, 1.0, hit)
        wgt = jnp.where(same, rw[:, k : k + 1], wgt)
    rank_rows, count = [], jnp.zeros((1, 1024), f32)
    for t in range(8):
        rank_rows.append(count)
        count = count + hit[t : t + 1]
    rank = jnp.concatenate(rank_rows, axis=0)
    sel = jnp.where(rank == lane_s.astype(f32), hit, 0.0)
    wsel = sel * wgt
    for q in range(4):
        ok = lane_q == q
        hsel[8 * q : 8 * q + 8, :] = jnp.where(ok, sel, 0.0)
        part = jnp.where(ok, wsel, 0.0)
        high = part.astype(bf16).astype(f32)
        hwgt[8 * q : 8 * q + 8, :] = high
        hwgt[32 + 8 * q : 40 + 8 * q, :] = part - high

    arrived(recv_b.at[pl.ds(0, 248)], 4)
    summed = []
    for j in range(8):
        total = recv_b[8 * j : 8 * j + 8, :].astype(f32)
        for k in range(1, 4):
            total = total + recv_b[64 * k + 8 * j : 64 * k + 8 * j + 8, :].astype(f32)
        summed.append(total.astype(bf16))

    def head(kind, h):
        return summed[kind * 2 + h // 4][:, 128 * (h % 4) : 128 * (h % 4) + 128]

    sub = lax.broadcasted_iota(jnp.int32, (8, 128), 0)
    for h in range(8):
        q_b = head(0, h)
        q = q_b.astype(f32)
        k = head(1, h).astype(f32) * (128 ** -0.5)
        v = head(2, h).astype(f32)
        o = head(3, h).astype(f32)
        keep, write = keep_old[:, h : h + 1], write_new[:, h : h + 1]
        wide = dot_nt(q_b, memb[h])
        read = jnp.zeros((8, 128), f32)
        for s in range(8):
            read = jnp.where(sub == s, wide[:, 128 * s : 128 * s + 128], read)
        n_h = nrm[:, h, :]
        score = write * jnp.sum(q * k, axis=-1, keepdims=True)
        den = keep * jnp.sum(n_h * q, axis=-1, keepdims=True) + score
        num = keep * read + score * v
        gated = jax.nn.sigmoid(o) * (num / jnp.maximum(jnp.abs(den), 1.0))
        g_a[pl.ds(pl.multiple_of(mine * 8, 8), 8), 128 * h : 128 * h + 128] = gated.astype(bf16)
        nn_out[:, h, :] = keep * n_h + write * k
        keep_b[:, h, :] = jnp.broadcast_to(keep, (8, 128))
        wv_b[:, h, :] = write * v
        k_b[:, h, :] = k

    line = [(dx, dc) for dx in (1, 3, 2, 0) for dc in (0, 1) if dx or dc]
    for dx, dc in line:
        send(rows(g_a, mine * 8, 8), rows(g_a, mine * 8, 8), 6, dev(0, 0, dx, dc))

    @pl.when(jx == jm)
    def _():
        arrived(ow_a.at[pl.ds(0, 240)], 5)

    @pl.when(jx != jm)
    def _():
        arrived(ow_a, 5)

    arrived(g_a.at[pl.ds(0, 56)], 6)
    out_c[...] = dot_nt(g_a[...], ow_a[...]).astype(bf16)
    recv_c[pl.ds(pl.multiple_of(jm * 8, 8), 8), :] = out_c[pl.ds(pl.multiple_of(mine * 8, 8), 8), :]
    for dx, dc in line:
        at = (xs[dx] * 2 + cs[dc]) * 8
        send(rows(out_c, at, 8), rows(recv_c, jm * 8, 8), 7, dev(0, 0, dx, dc))
    arrived(recv_c.at[pl.ds(0, 56)], 7)
    mixed = jnp.concatenate([recv_c[8 * p : 8 * p + 8, :].astype(f32) for p in range(8)], axis=1)
    after_mix = (residual + rms_scale(mixed, g_post[...])).astype(bf16).astype(f32)
    expert_input = rms_scale(after_mix, g_feed[...])

    quarters = jnp.concatenate([expert_input[:, 512 * q : 512 * q + 512] for q in range(4)], axis=0).astype(bf16)
    sel_t = jnp.transpose(hsel[...]).astype(bf16)
    d_out[...] = dot(sel_t, quarters).astype(bf16)
    for n, planes in enumerate(CHUNKS):
        for o in ALL:
            if o[0] in planes:
                target = dev(*o)
                send(rows(d_out, target * 8, 8), rows(d_in, me * 8, 8), 8 + n, target)
    d_in[pl.ds(pl.multiple_of(me * 8, 8), 8), :] = d_out[pl.ds(pl.multiple_of(me * 8, 8), 8), :]

    def renew(s, _):
        columns = jnp.transpose(wv_b[s])
        kept, keys = keep_b[s], k_b[s]
        for h in range(8):
            nm_out[s, h] = kept[h : h + 1, :] * mem[s, h] + columns[:, h : h + 1] * keys[h : h + 1, :]
        return 0

    lax.fori_loop(0, 8, renew, 0)

    for load in loads[1:4]:
        load.wait()
    x_in = expert_input.astype(bf16)
    s_hid = (jax.nn.silu(dot(x_in, sg[...])) * dot(x_in, su[...])).astype(bf16)
    shared = dot(s_hid, sd[...])
    for load in loads[4:]:
        load.wait()

    r_i = lax.broadcasted_iota(jnp.int32, (256, 256), 0)
    c_i = lax.broadcasted_iota(jnp.int32, (256, 256), 1)
    unmix = jnp.where(c_i == 4 * (r_i % 64) + r_i // 64, 1.0, 0.0).astype(bf16)
    remix = jnp.where(r_i == 4 * (c_i % 64) + c_i // 64, 1.0, 0.0).astype(bf16)
    for n, planes in enumerate(CHUNKS):
        arrived(d_in.at[pl.ds(0, 256 * len(planes) - (8 if 0 in planes else 0))], 8 + n)
        size = 64 * len(planes)
        for i, dz in enumerate(planes):
            block = d_in[pl.ds(pl.multiple_of(zs[-dz % 4] * 256, 256), 256), :]
            block = dot(unmix, block).astype(bf16)
            for q in range(4):
                u_in[64 * i : 64 * i + 64, 512 * q : 512 * q + 512] = block[64 * q : 64 * q + 64]

        def up_proj(k, _):
            cols = pl.ds(pl.multiple_of(k * 256, 256), 256)
            gate = dot(u_in[:size], eg[0, :, cols])
            up = dot(u_in[:size], eu[0, :, cols])
            hid[:size, cols] = (jax.nn.silu(gate) * up).astype(bf16)
            return 0

        lax.fori_loop(0, 2, up_proj, 0)

        def down_proj(q, _):
            cols = pl.ds(pl.multiple_of(q * 512, 512), 512)
            part = dot(hid[:size], ed[0, :, cols]).astype(bf16)
            for i in range(len(planes)):
                res[i, pl.ds(pl.multiple_of(q * 64, 64), 64), :] = part[64 * i : 64 * i + 64]
            return 0

        lax.fori_loop(0, 4, down_proj, 0)
        for i, dz in enumerate(planes):
            e_out[pl.ds(pl.multiple_of(zs[-dz % 4] * 256, 256), 256), :] = dot(remix, res[i]).astype(bf16)
        for o in ALL:
            if -o[0] % 4 in planes:
                target = dev(*o)
                send(rows(e_out, target * 8, 8), rows(e_in, me * 8, 8), 8 + len(CHUNKS), target)
    e_in[pl.ds(pl.multiple_of(me * 8, 8), 8), :] = e_out[pl.ds(pl.multiple_of(me * 8, 8), 8), :]

    sent(nb.at[pl.ds(0, 24)], 0)
    sent(w_a.at[pl.ds(0, 240)], 1)
    sent(tok_a.at[pl.ds(0, 224)], 2)
    sent(w_a.at[pl.ds(0, 256)], 3)
    sent(recv_b.at[pl.ds(0, 248)], 4)

    @pl.when(jx == jm)
    def _():
        sent(ow_a.at[pl.ds(0, 240)], 5)

    @pl.when(jx != jm)
    def _():
        sent(ow_a, 5)

    sent(g_a.at[pl.ds(0, 56)], 6)
    sent(recv_c.at[pl.ds(0, 56)], 7)
    for n, planes in enumerate(CHUNKS):
        sent(d_in.at[pl.ds(0, 256 * len(planes) - (8 if 0 in planes else 0))], 8 + n)

    arrived(e_in.at[pl.ds(0, 1016)], 8 + len(CHUNKS))
    comb = dot(hwgt[...].astype(bf16), e_in[...])
    comb = comb[:32] + comb[32:]
    routed = jnp.concatenate([comb[8 * q : 8 * q + 8] for q in range(4)], axis=1)
    nt_out[...] = (after_mix + rms_scale(routed + shared, g_out[...])).astype(bf16)
    sent(e_in.at[pl.ds(0, 1016)], 8 + len(CHUNKS))


def write_back(nm, nt, nn, ns, nm_out, nt_out, nn_out, ns_out, sem):
    copy = pltpu.make_async_copy(nm, nm_out, sem)
    copy.start()
    nt_out[...] = nt[...]
    nn_out[...] = nn[...]
    ns_out[...] = ns[...]
    copy.wait()


def on_device(
    tokens, premix_gain, postmix_gain, prefeed_gain, postfeed_gain, query_weight, key_weight,
    value_weight, outgate_weight, ingate_weight, forget_weight, ingate_bias, forget_bias,
    memory_state, normalizer, stabilizer, output_weight, expert_ids, route_weights, expert_gate,
    expert_up, expert_down, shared_gate, shared_up, shared_down,
):
    vm, hbm = pl.BlockSpec(memory_space=pltpu.VMEM), pl.BlockSpec(memory_space=pl.ANY)
    sd = jax.ShapeDtypeStruct
    buf = pltpu.VMEM
    nt, nn, ns, nm = pl.pallas_call(
        mega,
        out_shape=[
            buf((8, 2048), bf16),
            buf((8, 8, 128), f32),
            buf((8, 8), f32),
            buf((8, 8, 128, 128), f32),
        ],
        in_specs=[vm] * 13 + [hbm] + [vm] * 5 + [hbm] * 6,
        out_specs=[vm] * 4,
        scratch_shapes=[
            buf((8, 8, 128, 128), f32),
            buf((8, 1024, 128), bf16),
            buf((1, 2048, 512), bf16),
            buf((1, 2048, 512), bf16),
            buf((1, 512, 2048), bf16),
            buf((2048, 512), bf16),
            buf((2048, 512), bf16),
            buf((512, 2048), bf16),
            buf((32, 512), bf16),
            buf((128, 512), bf16),
            buf((256, 512), bf16),
            buf((512, 512), bf16),
            buf((256, 512), bf16),
            buf((256, 512), bf16),
            buf((256, 1024), bf16),
            buf((64, 1024), bf16),
            buf((64, 256), bf16),
            buf((64, 256), bf16),
            buf((32, 1024), f32),
            buf((64, 1024), f32),
            buf((1024, 512), bf16),
            buf((1024, 512), bf16),
            buf((256, 2048), bf16),
            buf((256, 512), bf16),
            buf((1024, 512), bf16),
            buf((1024, 512), bf16),
            buf((4, 256, 512), bf16),
            buf((8, 8, 128), f32),
            buf((8, 8, 128), f32),
            buf((8, 8, 128), f32),
            pltpu.SemaphoreType.DMA((7,)),
            pltpu.SemaphoreType.DMA((9 + len(CHUNKS),)),
            pltpu.SemaphoreType.DMA((9 + len(CHUNKS),)),
            pltpu.SemaphoreType.REGULAR,
        ],
        compiler_params=pltpu.CompilerParams(
            collective_id=0, has_side_effects=True, vmem_limit_bytes=58 * 2**20
        ),
    )(
        tokens,
        premix_gain.reshape(1, -1),
        postmix_gain.reshape(1, -1),
        prefeed_gain.reshape(1, -1),
        postfeed_gain.reshape(1, -1),
        query_weight,
        key_weight,
        value_weight,
        outgate_weight,
        ingate_weight.T,
        forget_weight.T,
        ingate_bias.reshape(1, -1),
        forget_bias.reshape(1, -1),
        memory_state,
        normalizer,
        stabilizer,
        output_weight.T,
        expert_ids,
        route_weights,
        expert_gate,
        expert_up,
        expert_down,
        shared_gate,
        shared_up,
        shared_down,
    )
    nm, nt, nn, ns = (pltpu.with_memory_space_constraint(a, pltpu.VMEM) for a in (nm, nt, nn, ns))
    nm, nt, nn, ns = pl.pallas_call(
        write_back,
        in_specs=[vm] * 4,
        out_specs=[hbm] + [vm] * 3,
        out_shape=[sd((8, 8, 128, 128), f32), sd((8, 2048), bf16), sd((8, 8, 128), f32), sd((8, 8), f32)],
        scratch_shapes=[pltpu.SemaphoreType.DMA],
        compiler_params=pltpu.CompilerParams(vmem_limit_bytes=8 * 2**20),
    )(nm, nt, nn, ns)
    return (nt, nm, nn, ns)


def solution(mesh):
    e2, e3, e4 = P("ep", None), P("ep", None, None), P("ep", None, None, None)
    in_specs = (
        e2, P(), P(), P(), P(), e2, e2, e2, e2, P(), P(), P(), P(), e4, e3, e2, P(None, "ep"),
        e2, e2, e3, e3, e3, P(), P(), P(),
    )
    return jax.shard_map(
        on_device, mesh=mesh, in_specs=in_specs, out_specs=(e2, e4, e3, e2), check_vma=False
    )
```

```python
import jax
import jax.numpy as jnp
from jax import lax
from jax.experimental import pallas as pl
from jax.experimental.pallas import tpu as pltpu
from jax.sharding import PartitionSpec as P

MESH = pl.DeviceIdType.MESH
epsilon = 1e-06
f32, bf16 = jnp.float32, jnp.bfloat16
N = 128


def rms_scale(values, gain_row):
    return (
        values * lax.rsqrt(jnp.mean(values * values, axis=-1, keepdims=True) + epsilon) * gain_row
    )


def dot(a, b):
    return jnp.dot(a, b, preferred_element_type=f32)


def dot_nt(a, b):
    return lax.dot_general(a, b, (((1,), (1,)), ((), ())), preferred_element_type=f32)


def rows(ref, at, count, step=8):
    return ref.at[pl.ds(pl.multiple_of(at, step), count)]


def spread(offsets):
    groups = {}
    for k, o in enumerate(sorted(offsets, key=lambda o: (o * 55) % 128)):
        c, x, y, z = o % 2, (o // 2) % 4, (o // 8) % 4, o // 32
        first = next((i, v) for i, v in ((2, x), (1, y), (0, z), (3, c)) if v)
        groups.setdefault(first, []).append((z, y, x, c))
    order, lists = [], list(groups.values())
    while any(lists):
        for entries in lists:
            if entries:
                order.append(entries.pop())
    return order


ALL = spread(range(1, N))
CHUNKS = ((1, 3), (0, 2))


def mega(
    tok, g_pre, g_post, g_feed, g_out, wq, wk, wv, wo, wi, wf, b_in, b_fg, mem_hbm, nrm, stab, owt,
    ids, rw, eg_hbm, eu_hbm, ed_hbm, sg_hbm, su_hbm, sd_hbm,
    nt_out, nn_out, ns_out, nm_out, mem, memb, eg, eu, ed, sg, su, sd,
    nb, wbuf, tok_a, w_a, out_b, recv_b, ow_a, g_a, out_c, recv_c, hsel, hwgt, d_out, d_in, u_in,
    e_out, e_in, res, keep_b, wv_b, k_b,
    sem_l, sem_s, sem_r, sem_k,
):
    me = lax.axis_index("ep")
    c, x, y, z = lax.rem(me, 2), lax.rem(lax.div(me, 2), 4), lax.rem(lax.div(me, 8), 4), lax.div(me, 32)
    xs = [lax.rem(x + d, 4) for d in range(4)]
    ys = [lax.rem(y + d, 4) for d in range(4)]
    zs = [lax.rem(z + d, 4) for d in range(4)]
    cs = [c, 1 - c]

    def dev(dz, dy, dx, dc):
        return zs[dz] * 32 + ys[dy] * 8 + xs[dx] * 2 + cs[dc]

    def send(src, dst, k, target):
        pltpu.make_async_remote_copy(
            src, dst, sem_s.at[k], sem_r.at[k], device_id=(target,), device_id_type=MESH
        ).start()

    def arrived(ref, k):
        pltpu.make_async_copy(ref, ref, sem_r.at[k]).wait()

    def sent(ref, k):
        pltpu.make_async_copy(ref, ref, sem_s.at[k]).wait()

    loads = [
        pltpu.make_async_copy(a, b, sem_l.at[k])
        for k, (a, b) in enumerate(
            (
                (mem_hbm, mem),
                (sg_hbm, sg),
                (su_hbm, su),
                (sd_hbm, sd),
                (eg_hbm, eg),
                (eu_hbm, eu),
                (ed_hbm, ed),
            )
        )
    ]
    loads[0].start()

    plane = [(0, dy, dx, 0) for dy in range(4) for dx in range(4) if dy or dx]
    zline = [(dz, 0, 0, 0) for dz in (1, 2, 3)]
    barrier = pltpu.get_barrier_semaphore()
    for o in sorted(plane + zline, key=lambda o: -sum(min(d, 4 - d) for d in o[:3])) + [(0, 0, 0, 1)]:
        pl.semaphore_signal(barrier, inc=1, device_id=(dev(*o),), device_id_type=MESH)
    for load in loads[1:]:
        load.start()

    residual = tok[...].astype(f32)
    normed = rms_scale(residual, g_pre[...]).astype(bf16)
    for k in range(4):
        nb[8 * k : 8 * k + 8, :] = normed[:, 512 * k : 512 * k + 512]
    for j, w in enumerate((wq, wk, wv, wo)):
        wbuf[32 * j : 32 * j + 16, :] = w[:, :512]
        wbuf[32 * j + 16 : 32 * j + 32, :] = w[:, 512:]

    half = lax.div(y, 2)
    gi = half * 4 + x
    slot_a = (gi * 4 + z) * 8
    tok_a[pl.ds(pl.multiple_of(slot_a, 8), 8), :] = nb[pl.ds(pl.multiple_of(z * 8, 8), 8), :]
    at_plane = (y * 4 + x) * 2 + c
    w_a[pl.ds(pl.multiple_of(at_plane * 16, 16), 16), :] = wbuf[
        pl.ds(pl.multiple_of(gi * 16, 16), 16), :
    ]
    pl.semaphore_wait(barrier, 19)

    for dz in (1, 2, 3):
        send(rows(nb, zs[dz] * 8, 8), rows(tok_a, slot_a, 8), 0, dev(dz, 0, 0, 0))
    for _, dy, dx, _ in [o for o in ALL if o[0] == 0 and o[3] == 0]:
        chunk = lax.div(ys[dy], 2) * 4 + xs[dx]
        send(
            rows(wbuf, chunk * 16, 16, 16),
            rows(w_a, at_plane * 16, 16, 16),
            1,
            dev(0, dy, dx, 0),
        )
    arrived(tok_a.at[pl.ds(0, 24)], 0)
    group = [(dy, dx) for dx in (1, 3, 2, 0) for dy in (0, 2) if dx or dy]
    for dy, dx in group:
        send(rows(tok_a, gi * 32, 32, 32), rows(tok_a, gi * 32, 32, 32), 2, dev(0, dy, dx, 0))
    pl.semaphore_signal(sem_k, inc=1, device_id=(dev(0, 0, 0, 1),), device_id_type=MESH)
    arrived(w_a.at[pl.ds(0, 240)], 1)
    for p in range(16):
        at = (2 * p + c) * 16
        send(rows(w_a, at, 16, 16), rows(w_a, at, 16, 16), 3, dev(0, 0, 0, 1))

    pl.semaphore_wait(sem_k, 1)

    input_pre = dot_nt(normed, wi[...]) + b_in[...]
    forget_pre = dot_nt(normed, wf[...]) + b_fg[...]
    log_sig = jnp.minimum(forget_pre, 0.0) - jnp.log1p(jnp.exp(-jnp.abs(forget_pre)))
    carried = log_sig + stab[...]
    next_stab = jnp.maximum(carried, input_pre)
    keep_old = jnp.exp(carried - next_stab)
    write_new = jnp.exp(input_pre - next_stab)
    ns_out[...] = next_stab
    loads[0].wait()

    def convert(s, _):
        for h in range(8):
            memb[h, pl.ds(pl.multiple_of(s * 128, 128), 128), :] = mem[s, h].astype(bf16)
        return 0

    lax.fori_loop(0, 8, convert, 0)

    arrived(tok_a.at[pl.ds(0, 224)], 2)
    arrived(w_a.at[pl.ds(0, 256)], 3)

    out_b[...] = dot(tok_a[...], w_a[...]).astype(bf16)
    slot_b = (z * 8 + gi) * 8
    recv_b[pl.ds(pl.multiple_of(slot_b, 8), 8), :] = out_b[pl.ds(pl.multiple_of(slot_a, 8), 8), :]
    for dz, dy, dx, dc in ALL:
        if dc == 0 and dy in (0, 2):
            at = ((lax.div(ys[dy], 2) * 4 + xs[dx]) * 4 + zs[dz]) * 8
            send(rows(out_b, at, 8), rows(recv_b, slot_b, 8), 4, dev(dz, dy, dx, 0))

    jx = lax.div(me, 16)
    jx_x, jx_c = lax.div(jx, 2), lax.rem(jx, 2)
    at_ow = lax.rem(me, 16) * 16
    mine = x * 2 + c
    jm = lax.rem(x + 8 - 2 * c - z - y, 4) * 2 + c
    for dz in range(4):
        for dy in range(4):
            target = zs[dz] * 32 + ys[dy] * 8 + lax.rem(jx_x + 2 * jx_c + zs[dz] + ys[dy], 4) * 2 + jx_c
            if dz == 0 and dy == 0:

                @pl.when(target == me)
                def _():
                    ow_a[pl.ds(pl.multiple_of(at_ow, 16), 16), :] = owt[...]

                @pl.when(target != me)
                def _():
                    send(owt, rows(ow_a, at_ow, 16, 16), 5, target)
            else:
                send(owt, rows(ow_a, at_ow, 16, 16), 5, target)

    lane = lax.broadcasted_iota(jnp.int32, (8, 1024), 1)
    lane_e, lane_s, lane_q = lane // 8, (lane // 4) % 2, lane % 4
    hit = jnp.zeros((8, 1024), f32)
    wgt = jnp.zeros((8, 1024), f32)
    for k in range(6):
        same = ids[:, k : k + 1] == lane_e
        hit = jnp.where(same, 1.0, hit)
        wgt = jnp.where(same, rw[:, k : k + 1], wgt)
    rank_rows, count = [], jnp.zeros((1, 1024), f32)
    for t in range(8):
        rank_rows.append(count)
        count = count + hit[t : t + 1]
    rank = jnp.concatenate(rank_rows, axis=0)
    sel = jnp.where(rank == lane_s.astype(f32), hit, 0.0)
    wsel = sel * wgt
    for q in range(4):
        ok = lane_q == q
        hsel[8 * q : 8 * q + 8, :] = jnp.where(ok, sel, 0.0)
        part = jnp.where(ok, wsel, 0.0)
        high = part.astype(bf16).astype(f32)
        hwgt[8 * q : 8 * q + 8, :] = high
        hwgt[32 + 8 * q : 40 + 8 * q, :] = part - high

    arrived(recv_b.at[pl.ds(0, 248)], 4)
    summed = []
    for j in range(8):
        total = recv_b[8 * j : 8 * j + 8, :].astype(f32)
        for k in range(1, 4):
            total = total + recv_b[64 * k + 8 * j : 64 * k + 8 * j + 8, :].astype(f32)
        summed.append(total.astype(bf16))

    def head(kind, h):
        return summed[kind * 2 + h // 4][:, 128 * (h % 4) : 128 * (h % 4) + 128]

    sub = lax.broadcasted_iota(jnp.int32, (8, 128), 0)
    for h in range(8):
        q_b = head(0, h)
        q = q_b.astype(f32)
        k = head(1, h).astype(f32) * (128 ** -0.5)
        v = head(2, h).astype(f32)
        o = head(3, h).astype(f32)
        keep, write = keep_old[:, h : h + 1], write_new[:, h : h + 1]
        wide = dot_nt(q_b, memb[h])
        read = jnp.zeros((8, 128), f32)
        for s in range(8):
            read = jnp.where(sub == s, wide[:, 128 * s : 128 * s + 128], read)
        n_h = nrm[:, h, :]
        score = write * jnp.sum(q * k, axis=-1, keepdims=True)
        den = keep * jnp.sum(n_h * q, axis=-1, keepdims=True) + score
        num = keep * read + score * v
        gated = jax.nn.sigmoid(o) * (num / jnp.maximum(jnp.abs(den), 1.0))
        g_a[pl.ds(pl.multiple_of(mine * 8, 8), 8), 128 * h : 128 * h + 128] = gated.astype(bf16)
        nn_out[:, h, :] = keep * n_h + write * k
        keep_b[:, h, :] = jnp.broadcast_to(keep, (8, 128))
        wv_b[:, h, :] = write * v
        k_b[:, h, :] = k

    line = [(dx, dc) for dx in (1, 3, 2, 0) for dc in (0, 1) if dx or dc]
    for dx, dc in line:
        send(rows(g_a, mine * 8, 8), rows(g_a, mine * 8, 8), 6, dev(0, 0, dx, dc))

    @pl.when(jx == jm)
    def _():
        arrived(ow_a.at[pl.ds(0, 240)], 5)

    @pl.when(jx != jm)
    def _():
        arrived(ow_a, 5)

    arrived(g_a.at[pl.ds(0, 56)], 6)
    out_c[...] = dot_nt(g_a[...], ow_a[...]).astype(bf16)
    recv_c[pl.ds(pl.multiple_of(jm * 8, 8), 8), :] = out_c[pl.ds(pl.multiple_of(mine * 8, 8), 8), :]
    for dx, dc in line:
        at = (xs[dx] * 2 + cs[dc]) * 8
        send(rows(out_c, at, 8), rows(recv_c, jm * 8, 8), 7, dev(0, 0, dx, dc))
    arrived(recv_c.at[pl.ds(0, 56)], 7)
    mixed = jnp.concatenate([recv_c[8 * p : 8 * p + 8, :].astype(f32) for p in range(8)], axis=1)
    after_mix = (residual + rms_scale(mixed, g_post[...])).astype(bf16).astype(f32)
    expert_input = rms_scale(after_mix, g_feed[...])

    quarters = jnp.concatenate([expert_input[:, 512 * q : 512 * q + 512] for q in range(4)], axis=0).astype(bf16)
    sel_t = jnp.transpose(hsel[...]).astype(bf16)
    d_out[...] = dot(sel_t, quarters).astype(bf16)
    for n, planes in enumerate(CHUNKS):
        for o in ALL:
            if o[0] in planes:
                target = dev(*o)
                send(rows(d_out, target * 8, 8), rows(d_in, me * 8, 8), 8 + n, target)
    d_in[pl.ds(pl.multiple_of(me * 8, 8), 8), :] = d_out[pl.ds(pl.multiple_of(me * 8, 8), 8), :]

    def renew(s, _):
        columns = jnp.transpose(wv_b[s])
        kept, keys = keep_b[s], k_b[s]
        for h in range(8):
            nm_out[s, h] = kept[h : h + 1, :] * mem[s, h] + columns[:, h : h + 1] * keys[h : h + 1, :]
        return 0

    lax.fori_loop(0, 8, renew, 0)

    for load in loads[1:4]:
        load.wait()
    x_in = expert_input.astype(bf16)
    s_hid = (jax.nn.silu(dot(x_in, sg[...])) * dot(x_in, su[...])).astype(bf16)
    shared = dot(s_hid, sd[...])
    for load in loads[4:]:
        load.wait()

    r_i = lax.broadcasted_iota(jnp.int32, (256, 256), 0)
    c_i = lax.broadcasted_iota(jnp.int32, (256, 256), 1)
    unmix = jnp.where(c_i == 4 * (r_i % 64) + r_i // 64, 1.0, 0.0).astype(bf16)
    remix = jnp.where(r_i == 4 * (c_i % 64) + c_i // 64, 1.0, 0.0).astype(bf16)
    for n, planes in enumerate(CHUNKS):
        arrived(d_in.at[pl.ds(0, 256 * len(planes) - (8 if 0 in planes else 0))], 8 + n)
        size = 64 * len(planes)
        for i, dz in enumerate(planes):
            block = d_in[pl.ds(pl.multiple_of(zs[-dz % 4] * 256, 256), 256), :]
            block = dot(unmix, block).astype(bf16)
            for q in range(4):
                u_in[64 * i : 64 * i + 64, 512 * q : 512 * q + 512] = block[64 * q : 64 * q + 64]

        gate, up = dot(u_in[:size], eg[0]), dot(u_in[:size], eu[0])
        hidden = (jax.nn.silu(gate) * up).astype(bf16)
        for q in range(4):
            part = dot(hidden, ed[0, :, 512 * q : 512 * q + 512]).astype(bf16)
            for i in range(len(planes)):
                res[i, 64 * q : 64 * q + 64, :] = part[64 * i : 64 * i + 64]
        for i, dz in enumerate(planes):
            e_out[pl.ds(pl.multiple_of(zs[-dz % 4] * 256, 256), 256), :] = dot(remix, res[i]).astype(bf16)
        for o in ALL:
            if -o[0] % 4 in planes:
                target = dev(*o)
                send(rows(e_out, target * 8, 8), rows(e_in, me * 8, 8), 8 + len(CHUNKS), target)
    e_in[pl.ds(pl.multiple_of(me * 8, 8), 8), :] = e_out[pl.ds(pl.multiple_of(me * 8, 8), 8), :]

    sent(nb.at[pl.ds(0, 24)], 0)
    sent(w_a.at[pl.ds(0, 240)], 1)
    sent(tok_a.at[pl.ds(0, 224)], 2)
    sent(w_a.at[pl.ds(0, 256)], 3)
    sent(recv_b.at[pl.ds(0, 248)], 4)

    @pl.when(jx == jm)
    def _():
        sent(ow_a.at[pl.ds(0, 240)], 5)

    @pl.when(jx != jm)
    def _():
        sent(ow_a, 5)

    sent(g_a.at[pl.ds(0, 56)], 6)
    sent(recv_c.at[pl.ds(0, 56)], 7)
    for n, planes in enumerate(CHUNKS):
        sent(d_in.at[pl.ds(0, 256 * len(planes) - (8 if 0 in planes else 0))], 8 + n)

    arrived(e_in.at[pl.ds(0, 1016)], 8 + len(CHUNKS))
    comb = dot(hwgt[...].astype(bf16), e_in[...])
    comb = comb[:32] + comb[32:]
    routed = jnp.concatenate([comb[8 * q : 8 * q + 8] for q in range(4)], axis=1)
    nt_out[...] = (after_mix + rms_scale(routed + shared, g_out[...])).astype(bf16)
    sent(e_in.at[pl.ds(0, 1016)], 8 + len(CHUNKS))


def write_back(nm, nt, nn, ns, nm_out, nt_out, nn_out, ns_out, sem):
    copy = pltpu.make_async_copy(nm, nm_out, sem)
    copy.start()
    nt_out[...] = nt[...]
    nn_out[...] = nn[...]
    ns_out[...] = ns[...]
    copy.wait()


def on_device(
    tokens, premix_gain, postmix_gain, prefeed_gain, postfeed_gain, query_weight, key_weight,
    value_weight, outgate_weight, ingate_weight, forget_weight, ingate_bias, forget_bias,
    memory_state, normalizer, stabilizer, output_weight, expert_ids, route_weights, expert_gate,
    expert_up, expert_down, shared_gate, shared_up, shared_down,
):
    vm, hbm = pl.BlockSpec(memory_space=pltpu.VMEM), pl.BlockSpec(memory_space=pl.ANY)
    sd = jax.ShapeDtypeStruct
    buf = pltpu.VMEM
    nt, nn, ns, nm = pl.pallas_call(
        mega,
        out_shape=[
            buf((8, 2048), bf16),
            buf((8, 8, 128), f32),
            buf((8, 8), f32),
            buf((8, 8, 128, 128), f32),
        ],
        in_specs=[vm] * 13 + [hbm] + [vm] * 5 + [hbm] * 6,
        out_specs=[vm] * 4,
        scratch_shapes=[
            buf((8, 8, 128, 128), f32),
            buf((8, 1024, 128), bf16),
            buf((1, 2048, 512), bf16),
            buf((1, 2048, 512), bf16),
            buf((1, 512, 2048), bf16),
            buf((2048, 512), bf16),
            buf((2048, 512), bf16),
            buf((512, 2048), bf16),
            buf((32, 512), bf16),
            buf((128, 512), bf16),
            buf((256, 512), bf16),
            buf((512, 512), bf16),
            buf((256, 512), bf16),
            buf((256, 512), bf16),
            buf((256, 1024), bf16),
            buf((64, 1024), bf16),
            buf((64, 256), bf16),
            buf((64, 256), bf16),
            buf((32, 1024), f32),
            buf((64, 1024), f32),
            buf((1024, 512), bf16),
            buf((1024, 512), bf16),
            buf((256, 2048), bf16),
            buf((1024, 512), bf16),
            buf((1024, 512), bf16),
            buf((4, 256, 512), bf16),
            buf((8, 8, 128), f32),
            buf((8, 8, 128), f32),
            buf((8, 8, 128), f32),
            pltpu.SemaphoreType.DMA((7,)),
            pltpu.SemaphoreType.DMA((9 + len(CHUNKS),)),
            pltpu.SemaphoreType.DMA((9 + len(CHUNKS),)),
            pltpu.SemaphoreType.REGULAR,
        ],
        compiler_params=pltpu.CompilerParams(
            collective_id=0, has_side_effects=True, vmem_limit_bytes=58 * 2**20
        ),
    )(
        tokens,
        premix_gain.reshape(1, -1),
        postmix_gain.reshape(1, -1),
        prefeed_gain.reshape(1, -1),
        postfeed_gain.reshape(1, -1),
        query_weight,
        key_weight,
        value_weight,
        outgate_weight,
        ingate_weight.T,
        forget_weight.T,
        ingate_bias.reshape(1, -1),
        forget_bias.reshape(1, -1),
        memory_state,
        normalizer,
        stabilizer,
        output_weight.T,
        expert_ids,
        route_weights,
        expert_gate,
        expert_up,
        expert_down,
        shared_gate,
        shared_up,
        shared_down,
    )
    nm, nt, nn, ns = (pltpu.with_memory_space_constraint(a, pltpu.VMEM) for a in (nm, nt, nn, ns))
    nm, nt, nn, ns = pl.pallas_call(
        write_back,
        in_specs=[vm] * 4,
        out_specs=[hbm] + [vm] * 3,
        out_shape=[sd((8, 8, 128, 128), f32), sd((8, 2048), bf16), sd((8, 8, 128), f32), sd((8, 8), f32)],
        scratch_shapes=[pltpu.SemaphoreType.DMA],
        compiler_params=pltpu.CompilerParams(vmem_limit_bytes=8 * 2**20),
    )(nm, nt, nn, ns)
    return (nt, nm, nn, ns)


def solution(mesh):
    e2, e3, e4 = P("ep", None), P("ep", None, None), P("ep", None, None, None)
    in_specs = (
        e2, P(), P(), P(), P(), e2, e2, e2, e2, P(), P(), P(), P(), e4, e3, e2, P(None, "ep"),
        e2, e2, e3, e3, e3, P(), P(), P(),
    )
    return jax.shard_map(
        on_device, mesh=mesh, in_specs=in_specs, out_specs=(e2, e4, e3, e2), check_vma=False
    )
```

```python
import jax
import jax.numpy as jnp
from jax import lax
from jax.experimental import pallas as pl
from jax.experimental.pallas import tpu as pltpu
from jax.sharding import PartitionSpec as P

MESH = pl.DeviceIdType.MESH
epsilon = 1e-06
f32, bf16 = jnp.float32, jnp.bfloat16
N = 128


def rms_scale(values, gain_row):
    return (
        values * lax.rsqrt(jnp.mean(values * values, axis=-1, keepdims=True) + epsilon) * gain_row
    )


def dot(a, b):
    return jnp.dot(a, b, preferred_element_type=f32)


def dot_nt(a, b):
    return lax.dot_general(a, b, (((1,), (1,)), ((), ())), preferred_element_type=f32)


def rows(ref, at, count, step=8):
    return ref.at[pl.ds(pl.multiple_of(at, step), count)]


def spread(offsets):
    groups = {}
    for k, o in enumerate(sorted(offsets, key=lambda o: (o * 55) % 128)):
        c, x, y, z = o % 2, (o // 2) % 4, (o // 8) % 4, o // 32
        first = next((i, v) for i, v in ((2, x), (1, y), (0, z), (3, c)) if v)
        groups.setdefault(first, []).append((z, y, x, c))
    order, lists = [], list(groups.values())
    while any(lists):
        for entries in lists:
            if entries:
                order.append(entries.pop())
    return order


ALL = spread(range(1, N))
CHUNKS = ((1, 3), (0, 2))


def mega(
    tok, g_pre, g_post, g_feed, g_out, wq, wk, wv, wo, wi, wf, b_in, b_fg, mem_hbm, nrm, stab, owt,
    ids, rw, eg_hbm, eu_hbm, ed_hbm, sg_hbm, su_hbm, sd_hbm,
    nt_out, nn_out, ns_out, nm_out, mem, memb, eg, eu, ed, sg, su, sd,
    nb, wbuf, tok_a, w_a, out_b, recv_b, ow_a, g_a, out_c, recv_c, hsel, hwgt, d_out, d_in, u_in,
    e_out, e_in, res, keep_b, wv_b, k_b,
    sem_l, sem_s, sem_r, sem_k,
):
    me = lax.axis_index("ep")
    c, x, y, z = lax.rem(me, 2), lax.rem(lax.div(me, 2), 4), lax.rem(lax.div(me, 8), 4), lax.div(me, 32)
    xs = [lax.rem(x + d, 4) for d in range(4)]
    ys = [lax.rem(y + d, 4) for d in range(4)]
    zs = [lax.rem(z + d, 4) for d in range(4)]
    cs = [c, 1 - c]

    def dev(dz, dy, dx, dc):
        return zs[dz] * 32 + ys[dy] * 8 + xs[dx] * 2 + cs[dc]

    def send(src, dst, k, target):
        pltpu.make_async_remote_copy(
            src, dst, sem_s.at[k], sem_r.at[k], device_id=(target,), device_id_type=MESH
        ).start()

    def arrived(ref, k):
        pltpu.make_async_copy(ref, ref, sem_r.at[k]).wait()

    def sent(ref, k):
        pltpu.make_async_copy(ref, ref, sem_s.at[k]).wait()

    loads = [
        pltpu.make_async_copy(a, b, sem_l.at[k])
        for k, (a, b) in enumerate(
            (
                (mem_hbm, mem),
                (sg_hbm, sg),
                (su_hbm, su),
                (sd_hbm, sd),
                (eg_hbm, eg),
                (eu_hbm, eu),
                (ed_hbm, ed),
            )
        )
    ]
    loads[0].start()

    plane = [(0, dy, dx, 0) for dy in range(4) for dx in range(4) if dy or dx]
    zline = [(dz, 0, 0, 0) for dz in (1, 2, 3)]
    barrier = pltpu.get_barrier_semaphore()
    for o in sorted(plane + zline, key=lambda o: -sum(min(d, 4 - d) for d in o[:3])) + [(0, 0, 0, 1)]:
        pl.semaphore_signal(barrier, inc=1, device_id=(dev(*o),), device_id_type=MESH)
    for load in loads[1:]:
        load.start()

    residual = tok[...].astype(f32)
    normed = rms_scale(residual, g_pre[...]).astype(bf16)
    for k in range(4):
        nb[8 * k : 8 * k + 8, :] = normed[:, 512 * k : 512 * k + 512]
    for j, w in enumerate((wq, wk, wv, wo)):
        wbuf[32 * j : 32 * j + 16, :] = w[:, :512]
        wbuf[32 * j + 16 : 32 * j + 32, :] = w[:, 512:]

    half = lax.div(y, 2)
    gi = half * 4 + x
    slot_a = (gi * 4 + z) * 8
    tok_a[pl.ds(pl.multiple_of(slot_a, 8), 8), :] = nb[pl.ds(pl.multiple_of(z * 8, 8), 8), :]
    at_plane = (y * 4 + x) * 2 + c
    w_a[pl.ds(pl.multiple_of(at_plane * 16, 16), 16), :] = wbuf[
        pl.ds(pl.multiple_of(gi * 16, 16), 16), :
    ]
    pl.semaphore_wait(barrier, 19)

    for dz in (1, 2, 3):
        send(rows(nb, zs[dz] * 8, 8), rows(tok_a, slot_a, 8), 0, dev(dz, 0, 0, 0))
    for _, dy, dx, _ in [o for o in ALL if o[0] == 0 and o[3] == 0]:
        chunk = lax.div(ys[dy], 2) * 4 + xs[dx]
        send(
            rows(wbuf, chunk * 16, 16, 16),
            rows(w_a, at_plane * 16, 16, 16),
            1,
            dev(0, dy, dx, 0),
        )
    arrived(tok_a.at[pl.ds(0, 24)], 0)
    group = [(dy, dx) for dx in (1, 3, 2, 0) for dy in (0, 2) if dx or dy]
    for dy, dx in group:
        send(rows(tok_a, gi * 32, 32, 32), rows(tok_a, gi * 32, 32, 32), 2, dev(0, dy, dx, 0))
    pl.semaphore_signal(sem_k, inc=1, device_id=(dev(0, 0, 0, 1),), device_id_type=MESH)
    arrived(w_a.at[pl.ds(0, 240)], 1)
    for p in range(16):
        at = (2 * p + c) * 16
        send(rows(w_a, at, 16, 16), rows(w_a, at, 16, 16), 3, dev(0, 0, 0, 1))

    pl.semaphore_wait(sem_k, 1)

    input_pre = dot_nt(normed, wi[...]) + b_in[...]
    forget_pre = dot_nt(normed, wf[...]) + b_fg[...]
    log_sig = jnp.minimum(forget_pre, 0.0) - jnp.log1p(jnp.exp(-jnp.abs(forget_pre)))
    carried = log_sig + stab[...]
    next_stab = jnp.maximum(carried, input_pre)
    keep_old = jnp.exp(carried - next_stab)
    write_new = jnp.exp(input_pre - next_stab)
    ns_out[...] = next_stab
    loads[0].wait()

    def convert(s, _):
        for h in range(8):
            memb[h, pl.ds(pl.multiple_of(s * 128, 128), 128), :] = mem[s, h].astype(bf16)
        return 0

    lax.fori_loop(0, 8, convert, 0)

    arrived(tok_a.at[pl.ds(0, 224)], 2)
    arrived(w_a.at[pl.ds(0, 256)], 3)

    out_b[...] = dot(tok_a[...], w_a[...]).astype(bf16)
    slot_b = (z * 8 + gi) * 8
    recv_b[pl.ds(pl.multiple_of(slot_b, 8), 8), :] = out_b[pl.ds(pl.multiple_of(slot_a, 8), 8), :]
    for dz, dy, dx, dc in ALL:
        if dc == 0 and dy in (0, 2):
            at = ((lax.div(ys[dy], 2) * 4 + xs[dx]) * 4 + zs[dz]) * 8
            send(rows(out_b, at, 8), rows(recv_b, slot_b, 8), 4, dev(dz, dy, dx, 0))

    jx = lax.div(me, 16)
    jx_x, jx_c = lax.div(jx, 2), lax.rem(jx, 2)
    at_ow = lax.rem(me, 16) * 16
    mine = x * 2 + c
    jm = lax.rem(x + 8 - 2 * c - z - y, 4) * 2 + c
    for dz in range(4):
        for dy in range(4):
            target = zs[dz] * 32 + ys[dy] * 8 + lax.rem(jx_x + 2 * jx_c + zs[dz] + ys[dy], 4) * 2 + jx_c
            if dz == 0 and dy == 0:

                @pl.when(target == me)
                def _():
                    ow_a[pl.ds(pl.multiple_of(at_ow, 16), 16), :] = owt[...]

                @pl.when(target != me)
                def _():
                    send(owt, rows(ow_a, at_ow, 16, 16), 5, target)
            else:
                send(owt, rows(ow_a, at_ow, 16, 16), 5, target)

    lane = lax.broadcasted_iota(jnp.int32, (8, 1024), 1)
    lane_e, lane_s, lane_q = lane // 8, (lane // 4) % 2, lane % 4
    hit = jnp.zeros((8, 1024), f32)
    wgt = jnp.zeros((8, 1024), f32)
    for k in range(6):
        same = ids[:, k : k + 1] == lane_e
        hit = jnp.where(same, 1.0, hit)
        wgt = jnp.where(same, rw[:, k : k + 1], wgt)
    rank_rows, count = [], jnp.zeros((1, 1024), f32)
    for t in range(8):
        rank_rows.append(count)
        count = count + hit[t : t + 1]
    rank = jnp.concatenate(rank_rows, axis=0)
    sel = jnp.where(rank == lane_s.astype(f32), hit, 0.0)
    wsel = sel * wgt
    for q in range(4):
        ok = lane_q == q
        hsel[8 * q : 8 * q + 8, :] = jnp.where(ok, sel, 0.0)
        part = jnp.where(ok, wsel, 0.0)
        high = part.astype(bf16).astype(f32)
        hwgt[8 * q : 8 * q + 8, :] = high
        hwgt[32 + 8 * q : 40 + 8 * q, :] = part - high

    arrived(recv_b.at[pl.ds(0, 248)], 4)
    summed = []
    for j in range(8):
        total = recv_b[8 * j : 8 * j + 8, :].astype(f32)
        for k in range(1, 4):
            total = total + recv_b[64 * k + 8 * j : 64 * k + 8 * j + 8, :].astype(f32)
        summed.append(total.astype(bf16))

    def head(kind, h):
        return summed[kind * 2 + h // 4][:, 128 * (h % 4) : 128 * (h % 4) + 128]

    sub = lax.broadcasted_iota(jnp.int32, (8, 128), 0)
    line = [(dx, dc) for dx in (1, 3, 2, 0) for dc in (0, 1) if dx or dc]
    later = []
    for h in range(8):
        q_b = head(0, h)
        q = q_b.astype(f32)
        k = head(1, h).astype(f32) * (128 ** -0.5)
        v = head(2, h).astype(f32)
        o = head(3, h).astype(f32)
        keep, write = keep_old[:, h : h + 1], write_new[:, h : h + 1]
        wide = dot_nt(q_b, memb[h])
        read = jnp.zeros((8, 128), f32)
        for s in range(8):
            read = jnp.where(sub == s, wide[:, 128 * s : 128 * s + 128], read)
        n_h = nrm[:, h, :]
        score = write * jnp.sum(q * k, axis=-1, keepdims=True)
        den = keep * jnp.sum(n_h * q, axis=-1, keepdims=True) + score
        num = keep * read + score * v
        gated = jax.nn.sigmoid(o) * (num / jnp.maximum(jnp.abs(den), 1.0))
        g_a[pl.ds(pl.multiple_of(mine * 8, 8), 8), 128 * h : 128 * h + 128] = gated.astype(bf16)
        later.append((keep, write, n_h, k, v))
    for dx, dc in line:
        send(rows(g_a, mine * 8, 8), rows(g_a, mine * 8, 8), 6, dev(0, 0, dx, dc))
    for h, (keep, write, n_h, k, v) in enumerate(later):
        nn_out[:, h, :] = keep * n_h + write * k
        keep_b[:, h, :] = jnp.broadcast_to(keep, (8, 128))
        wv_b[:, h, :] = write * v
        k_b[:, h, :] = k


    @pl.when(jx == jm)
    def _():
        arrived(ow_a.at[pl.ds(0, 240)], 5)

    @pl.when(jx != jm)
    def _():
        arrived(ow_a, 5)

    arrived(g_a.at[pl.ds(0, 56)], 6)
    out_c[...] = dot_nt(g_a[...], ow_a[...]).astype(bf16)
    recv_c[pl.ds(pl.multiple_of(jm * 8, 8), 8), :] = out_c[pl.ds(pl.multiple_of(mine * 8, 8), 8), :]
    for dx, dc in line:
        at = (xs[dx] * 2 + cs[dc]) * 8
        send(rows(out_c, at, 8), rows(recv_c, jm * 8, 8), 7, dev(0, 0, dx, dc))
    arrived(recv_c.at[pl.ds(0, 56)], 7)
    mixed = jnp.concatenate([recv_c[8 * p : 8 * p + 8, :].astype(f32) for p in range(8)], axis=1)
    after_mix = (residual + rms_scale(mixed, g_post[...])).astype(bf16).astype(f32)
    expert_input = rms_scale(after_mix, g_feed[...])

    quarters = jnp.concatenate([expert_input[:, 512 * q : 512 * q + 512] for q in range(4)], axis=0).astype(bf16)
    sel_t = jnp.transpose(hsel[...]).astype(bf16)
    d_out[...] = dot(sel_t, quarters).astype(bf16)
    for n, planes in enumerate(CHUNKS):
        for o in ALL:
            if o[0] in planes:
                target = dev(*o)
                send(rows(d_out, target * 8, 8), rows(d_in, me * 8, 8), 8 + n, target)
    d_in[pl.ds(pl.multiple_of(me * 8, 8), 8), :] = d_out[pl.ds(pl.multiple_of(me * 8, 8), 8), :]

    def renew(s, _):
        columns = jnp.transpose(wv_b[s])
        kept, keys = keep_b[s], k_b[s]
        for h in range(8):
            nm_out[s, h] = kept[h : h + 1, :] * mem[s, h] + columns[:, h : h + 1] * keys[h : h + 1, :]
        return 0

    lax.fori_loop(0, 8, renew, 0)

    for load in loads[1:4]:
        load.wait()
    x_in = expert_input.astype(bf16)
    s_hid = (jax.nn.silu(dot(x_in, sg[...])) * dot(x_in, su[...])).astype(bf16)
    shared = dot(s_hid, sd[...])
    for load in loads[4:]:
        load.wait()

    r_i = lax.broadcasted_iota(jnp.int32, (256, 256), 0)
    c_i = lax.broadcasted_iota(jnp.int32, (256, 256), 1)
    unmix = jnp.where(c_i == 4 * (r_i % 64) + r_i // 64, 1.0, 0.0).astype(bf16)
    remix = jnp.where(r_i == 4 * (c_i % 64) + c_i // 64, 1.0, 0.0).astype(bf16)
    for n, planes in enumerate(CHUNKS):
        arrived(d_in.at[pl.ds(0, 256 * len(planes) - (8 if 0 in planes else 0))], 8 + n)
        size = 64 * len(planes)
        for i, dz in enumerate(planes):
            block = d_in[pl.ds(pl.multiple_of(zs[-dz % 4] * 256, 256), 256), :]
            block = dot(unmix, block).astype(bf16)
            for q in range(4):
                u_in[64 * i : 64 * i + 64, 512 * q : 512 * q + 512] = block[64 * q : 64 * q + 64]

        gate, up = dot(u_in[:size], eg[0]), dot(u_in[:size], eu[0])
        hidden = (jax.nn.silu(gate) * up).astype(bf16)
        for q in range(4):
            part = dot(hidden, ed[0, :, 512 * q : 512 * q + 512]).astype(bf16)
            for i in range(len(planes)):
                res[i, 64 * q : 64 * q + 64, :] = part[64 * i : 64 * i + 64]
        for i, dz in enumerate(planes):
            e_out[pl.ds(pl.multiple_of(zs[-dz % 4] * 256, 256), 256), :] = dot(remix, res[i]).astype(bf16)
        for o in ALL:
            if -o[0] % 4 in planes:
                target = dev(*o)
                send(rows(e_out, target * 8, 8), rows(e_in, me * 8, 8), 8 + len(CHUNKS), target)
    e_in[pl.ds(pl.multiple_of(me * 8, 8), 8), :] = e_out[pl.ds(pl.multiple_of(me * 8, 8), 8), :]

    sent(nb.at[pl.ds(0, 24)], 0)
    sent(w_a.at[pl.ds(0, 240)], 1)
    sent(tok_a.at[pl.ds(0, 224)], 2)
    sent(w_a.at[pl.ds(0, 256)], 3)
    sent(recv_b.at[pl.ds(0, 248)], 4)

    @pl.when(jx == jm)
    def _():
        sent(ow_a.at[pl.ds(0, 240)], 5)

    @pl.when(jx != jm)
    def _():
        sent(ow_a, 5)

    sent(g_a.at[pl.ds(0, 56)], 6)
    sent(recv_c.at[pl.ds(0, 56)], 7)
    for n, planes in enumerate(CHUNKS):
        sent(d_in.at[pl.ds(0, 256 * len(planes) - (8 if 0 in planes else 0))], 8 + n)

    arrived(e_in.at[pl.ds(0, 1016)], 8 + len(CHUNKS))
    comb = dot(hwgt[...].astype(bf16), e_in[...])
    comb = comb[:32] + comb[32:]
    routed = jnp.concatenate([comb[8 * q : 8 * q + 8] for q in range(4)], axis=1)
    nt_out[...] = (after_mix + rms_scale(routed + shared, g_out[...])).astype(bf16)
    sent(e_in.at[pl.ds(0, 1016)], 8 + len(CHUNKS))


def write_back(nm, nt, nn, ns, nm_out, nt_out, nn_out, ns_out, sem):
    copy = pltpu.make_async_copy(nm, nm_out, sem)
    copy.start()
    nt_out[...] = nt[...]
    nn_out[...] = nn[...]
    ns_out[...] = ns[...]
    copy.wait()


def on_device(
    tokens, premix_gain, postmix_gain, prefeed_gain, postfeed_gain, query_weight, key_weight,
    value_weight, outgate_weight, ingate_weight, forget_weight, ingate_bias, forget_bias,
    memory_state, normalizer, stabilizer, output_weight, expert_ids, route_weights, expert_gate,
    expert_up, expert_down, shared_gate, shared_up, shared_down,
):
    vm, hbm = pl.BlockSpec(memory_space=pltpu.VMEM), pl.BlockSpec(memory_space=pl.ANY)
    sd = jax.ShapeDtypeStruct
    buf = pltpu.VMEM
    nt, nn, ns, nm = pl.pallas_call(
        mega,
        out_shape=[
            buf((8, 2048), bf16),
            buf((8, 8, 128), f32),
            buf((8, 8), f32),
            buf((8, 8, 128, 128), f32),
        ],
        in_specs=[vm] * 13 + [hbm] + [vm] * 5 + [hbm] * 6,
        out_specs=[vm] * 4,
        scratch_shapes=[
            buf((8, 8, 128, 128), f32),
            buf((8, 1024, 128), bf16),
            buf((1, 2048, 512), bf16),
            buf((1, 2048, 512), bf16),
            buf((1, 512, 2048), bf16),
            buf((2048, 512), bf16),
            buf((2048, 512), bf16),
            buf((512, 2048), bf16),
            buf((32, 512), bf16),
            buf((128, 512), bf16),
            buf((256, 512), bf16),
            buf((512, 512), bf16),
            buf((256, 512), bf16),
            buf((256, 512), bf16),
            buf((256, 1024), bf16),
            buf((64, 1024), bf16),
            buf((64, 256), bf16),
            buf((64, 256), bf16),
            buf((32, 1024), f32),
            buf((64, 1024), f32),
            buf((1024, 512), bf16),
            buf((1024, 512), bf16),
            buf((256, 2048), bf16),
            buf((1024, 512), bf16),
            buf((1024, 512), bf16),
            buf((4, 256, 512), bf16),
            buf((8, 8, 128), f32),
            buf((8, 8, 128), f32),
            buf((8, 8, 128), f32),
            pltpu.SemaphoreType.DMA((7,)),
            pltpu.SemaphoreType.DMA((9 + len(CHUNKS),)),
            pltpu.SemaphoreType.DMA((9 + len(CHUNKS),)),
            pltpu.SemaphoreType.REGULAR,
        ],
        compiler_params=pltpu.CompilerParams(
            collective_id=0, has_side_effects=True, vmem_limit_bytes=58 * 2**20
        ),
    )(
        tokens,
        premix_gain.reshape(1, -1),
        postmix_gain.reshape(1, -1),
        prefeed_gain.reshape(1, -1),
        postfeed_gain.reshape(1, -1),
        query_weight,
        key_weight,
        value_weight,
        outgate_weight,
        ingate_weight.T,
        forget_weight.T,
        ingate_bias.reshape(1, -1),
        forget_bias.reshape(1, -1),
        memory_state,
        normalizer,
        stabilizer,
        output_weight.T,
        expert_ids,
        route_weights,
        expert_gate,
        expert_up,
        expert_down,
        shared_gate,
        shared_up,
        shared_down,
    )
    nm, nt, nn, ns = (pltpu.with_memory_space_constraint(a, pltpu.VMEM) for a in (nm, nt, nn, ns))
    nm, nt, nn, ns = pl.pallas_call(
        write_back,
        in_specs=[vm] * 4,
        out_specs=[hbm] + [vm] * 3,
        out_shape=[sd((8, 8, 128, 128), f32), sd((8, 2048), bf16), sd((8, 8, 128), f32), sd((8, 8), f32)],
        scratch_shapes=[pltpu.SemaphoreType.DMA],
        compiler_params=pltpu.CompilerParams(vmem_limit_bytes=8 * 2**20),
    )(nm, nt, nn, ns)
    return (nt, nm, nn, ns)


def solution(mesh):
    e2, e3, e4 = P("ep", None), P("ep", None, None), P("ep", None, None, None)
    in_specs = (
        e2, P(), P(), P(), P(), e2, e2, e2, e2, P(), P(), P(), P(), e4, e3, e2, P(None, "ep"),
        e2, e2, e3, e3, e3, P(), P(), P(),
    )
    return jax.shard_map(
        on_device, mesh=mesh, in_specs=in_specs, out_specs=(e2, e4, e3, e2), check_vma=False
    )
```
